512 devices in a mesh: sp: 32 (over z, core), tp: 16 (over y, x).
Axes of the slice: x: 4, y: 4, z: 16, core: 2. Of those that a mesh axis runs over, the one named last changes fastest.
Arguments:
- queries: bfloat16 [8192, 2048], P('sp', 'tp'), may hold values from -8 to 8
- key_rows: bfloat16 [8192, 1024], P('sp', 'tp'), may hold values from -8 to 8
- values: bfloat16 [8192, 1024], P('sp', 'tp'), may hold values from -6 to 6
- sink_logits: float32 [32], P('tp'), may hold values from 2 to 6
- residual: bfloat16 [8192, 2048], P(('sp', 'tp')), may hold values from -6 to 6
- out_weight: bfloat16 [2048, 2048], P('tp'), may hold values from -0.125 to 0.125
- norm_gain: float32 [2048], replicated, may hold values from 0.1 to 1.9
- expert_ids: int32 [8192, 2], P('sp'), may hold values from 0 to 31, as said below
- route_weight: float32 [8192, 2], P('sp'), may hold values from 0.2 to 1
- gate_proj: bfloat16 [32, 2048, 4096], P('sp', None, 'tp'), may hold values from -0.125 to 0.125
- up_proj: bfloat16 [32, 2048, 4096], P('sp', None, 'tp'), may hold values from -0.125 to 0.125
- down_proj: bfloat16 [32, 4096, 2048], P('sp', 'tp'), may hold values from -0.09375 to 0.09375
Outputs:
- mixed_out: bfloat16 [8192, 2048], P(('sp', 'tp'))
The draws below stay inside these ranges and needn't reach their ends.
Inputs may be any that keep to these rules, and one draw needn't show every extreme that they name: `expert_ids`: the two entries of a row are different experts of one group: experts g * 8 to g * 8 + 7 for a group g below 4. In each aligned block of 16 rows (the rows of one device) no expert is named more than 2 times, and one expert is named exactly 2 times in every block.
All inputs are finite; a program needn't handle non-finite values.
Results may differ from the reference program's by a relative error of at most 0.014.
Values may be sent and summed in bfloat16 or wider, within the bound.
No kernel may reach another device: no remote copies, remote signals or barrier semaphores. Data moves between devices by JAX's collectives and lax.ppermute only.
A program may use at most 64 MiB of HBM per device.

```python
import math
import jax
import jax.numpy as jnp
from jax import lax

D = 2048
HEAD = 64
QH = 32
KVH = 16
WINDOW = 128
FFE = 4096
TOK_SP = 256
CAP = 2
SEQ = 8192
EXPERTS = 32
INNER = 8
N_SP = 32
N_TP = 16


def draw_queries(key, part):
    sampled = jnp.clip(jax.random.normal(jax.random.fold_in(key, 3), (SEQ, QH * HEAD), jnp.float32), -5.5, 5.5)
    return sampled.astype(jnp.bfloat16)


def draw_key_rows(key, part):
    sampled = jnp.clip(jax.random.normal(jax.random.fold_in(key, 8), (SEQ, KVH * HEAD), jnp.float32), -5.5, 5.5)
    return sampled.astype(jnp.bfloat16)


def draw_expert_ids(key, part):
    rows_per = TOK_SP // N_TP
    block_count = SEQ // rows_per
    favour = jax.random.randint(jax.random.fold_in(key, 5), (N_SP,), 0, 1500)
    jitter = jax.random.randint(jax.random.fold_in(key, 6), (block_count, rows_per, 2, N_SP), 0, 1000)
    forced = jax.random.randint(jax.random.fold_in(key, 7), (), 0, N_SP)
    labels = jnp.arange(N_SP, dtype=jnp.int32)
    family = labels // INNER
    same_family = (family[:, None] == family[None, :]).astype(jnp.int32)

    def one_block(block_jitter):

        def place(counts, entry_item):
            position, random_draws = entry_item
            has_room = (counts < CAP).astype(jnp.int32)
            family_room = jnp.sum(same_family * has_room[None, :], 1)
            usable = (has_room > 0) & (family_room >= 2)
            ranking = (random_draws[0] + favour) * N_SP + labels
            ranking = jnp.where((labels == forced) & (position < CAP), 100000000, ranking)
            ranking = jnp.where(usable, ranking, -1)
            first_pick = jnp.argmax(ranking).astype(jnp.int32)
            usable_two = (has_room > 0) & (family == family[first_pick]) & (labels != first_pick)
            ranking_two = jnp.where(usable_two, (random_draws[1] + favour) * N_SP + labels, -1)
            second = jnp.argmax(ranking_two).astype(jnp.int32)
            counts = counts + (labels == first_pick).astype(jnp.int32) + (labels == second).astype(jnp.int32)
            return (counts, jnp.stack([first_pick, second]))
        ignored, chosen = lax.scan(place, jnp.zeros((N_SP,), jnp.int32), (jnp.arange(rows_per, dtype=jnp.int32), block_jitter))
        return chosen
    return jax.vmap(one_block)(jitter).reshape(SEQ, 2).astype(jnp.int32)


def block_levels(key, dims, split, smallest, top_value):
    loudness, own = 1.0, jax.random.fold_in(key, 6)
    for axis_at, parts in split:
        draws = jnp.exp(jax.random.uniform(jax.random.fold_in(own, axis_at), (parts,), jnp.float32, smallest / len(split), top_value / len(split)))
        loudness = loudness * jnp.repeat(draws, dims[axis_at] // parts).reshape([-1 if axis == axis_at else 1 for axis in range(len(dims))])
    return loudness


def bell_draw(key, dims, spread, reach, pieces=(), kind=jnp.bfloat16):
    values = spread * jax.random.normal(key, dims, jnp.float32)
    if pieces:
        values = values * block_levels(key, dims, pieces, -0.22, 0.18)
    return jnp.clip(values, -reach, reach).astype(kind)


def setup_inputs(seed: int = 0) -> dict:
    splits = jax.random.split(jax.random.key(seed), 13)
    return {
        "queries": draw_queries(jax.random.fold_in(splits[12], 71), 0),
        "key_rows": draw_key_rows(jax.random.fold_in(splits[12], 71), 0),
        "values": bell_draw(splits[2], (SEQ, KVH * HEAD), 1.0, 6.0, ((0, 32), (1, 16))),
        "sink_logits": jnp.clip(2.0 + 4.0 * jax.random.uniform(splits[3], (QH,), jnp.float32) ** block_levels(splits[3], (QH,), ((0, 16),), -0.2, 0.2), 2.0, 6.0),
        "residual": bell_draw(splits[4], (SEQ, D), 1.0, 6.0, ((0, 512),)),
        "out_weight": bell_draw(splits[5], (QH * HEAD, D), (QH * HEAD) ** -0.5, 0.125, ((0, 16),)),
        "norm_gain": jnp.clip(1.0 + 0.18 * jax.random.normal(splits[6], (D,), jnp.float32), 0.1, 1.9),
        "expert_ids": draw_expert_ids(jax.random.fold_in(splits[12], 71), 0),
        "route_weight": jnp.clip(jnp.exp(math.log(1.0) - 1.609438 * jax.random.uniform(splits[8], (SEQ, 2), jnp.float32) ** block_levels(splits[8], (SEQ, 2), ((0, 32),), -0.2, 0.2)), 0.2, 1.0),
        "gate_proj": bell_draw(splits[9], (EXPERTS, D, FFE), D ** -0.5, 0.125, ((0, 32), (2, 16))),
        "up_proj": bell_draw(splits[10], (EXPERTS, D, FFE), D ** -0.5, 0.125, ((0, 32), (2, 16))),
        "down_proj": bell_draw(splits[11], (EXPERTS, FFE, D), FFE ** -0.5, 0.09375, ((0, 32), (1, 16))),
    }


norm_epsilon = 1e-06

def rotary(values_in, positions, head_count):
    halfway = HEAD // 2
    frequency = 10000.0 ** (-jnp.arange(halfway, dtype=jnp.float32) * 2.0 / HEAD)
    angles = positions.astype(jnp.float32)[:, None] * frequency[None, :]
    cosine = jnp.cos(angles)[:, None, :]
    sine_part = jnp.sin(angles)[:, None, :]
    reshaped = values_in.astype(jnp.float32).reshape(values_in.shape[0], head_count, HEAD)
    front_part = reshaped[..., :halfway]
    back_part = reshaped[..., halfway:]
    turned = jnp.concatenate([front_part * cosine - back_part * sine_part, back_part * cosine + front_part * sine_part], -1)
    return turned.astype(jnp.bfloat16)

def attend(query_blocks, key_pairs, value_pairs, sink_grid, key_start):
    block_count = query_blocks.shape[0]
    window_len = query_blocks.shape[1]
    scores = jnp.einsum('bqkgd,bskd->bkgqs', query_blocks.astype(jnp.float32), key_pairs.astype(jnp.float32)) * HEAD ** (-0.5)
    row_idx = jnp.arange(window_len)[:, None]
    col_idx = jnp.arange(2 * window_len)[None, :]
    distance = row_idx - col_idx + window_len
    key_pos = key_start + jnp.arange(block_count)[:, None, None] * window_len + col_idx[None]
    allowed = (distance >= 0)[None] & (distance < window_len)[None] & (key_pos >= 0)
    scores = jnp.where(allowed[:, None, None], scores, -jnp.inf)
    sink_full = sink_grid.astype(jnp.float32)[None, :, :, None]
    highest = jnp.maximum(lax.optimization_barrier(jnp.max(scores, -1)), sink_full)
    exp_scores = jnp.exp(scores - highest[..., None])
    denominator = lax.optimization_barrier(jnp.sum(exp_scores, -1)) + jnp.exp(sink_full - highest)
    probs = lax.optimization_barrier(exp_scores.astype(jnp.bfloat16)).astype(jnp.float32)
    weighted = jnp.einsum('bkgqs,bskd->bkgqd', probs, value_pairs.astype(jnp.float32))
    normalized = weighted / denominator[..., None]
    return jnp.transpose(normalized, (0, 3, 1, 2, 4)).astype(jnp.bfloat16).reshape(block_count * window_len, -1)

def reference(queries, key_rows, values, sink_logits, residual, out_weight, norm_gain, expert_ids, route_weight, gate_proj, up_proj, down_proj):
    seq_len = queries.shape[0]
    positions = jnp.arange(seq_len, dtype=jnp.int32)
    rot_query = rotary(queries, positions, QH)
    rot_key = rotary(key_rows, positions, KVH)
    group_size = QH // KVH
    block_count = seq_len // WINDOW
    padding = jnp.zeros((WINDOW, KVH, HEAD), jnp.bfloat16)
    key_blocks = jnp.concatenate([padding, rot_key], 0).reshape(block_count + 1, WINDOW, KVH, HEAD)
    value_blocks = jnp.concatenate([padding, values.reshape(seq_len, KVH, HEAD)], 0).reshape(block_count + 1, WINDOW, KVH, HEAD)
    key_pairs = jnp.concatenate([key_blocks[:-1], key_blocks[1:]], 1)
    value_pairs = jnp.concatenate([value_blocks[:-1], value_blocks[1:]], 1)
    query_blocks = rot_query.reshape(block_count, WINDOW, KVH, group_size, HEAD)
    sink_grid = sink_logits.reshape(KVH, group_size)

    def one_head(entry_item):
        query_part, key_part, value_part, sink_part = entry_item
        return attend(query_part[:, :, None], key_part[:, :, None], value_part[:, :, None], sink_part[None], -WINDOW)
    per_head = lax.map(one_head, (jnp.moveaxis(query_blocks, 2, 0), jnp.moveaxis(key_pairs, 2, 0), jnp.moveaxis(value_pairs, 2, 0), sink_grid))
    attended = jnp.moveaxis(per_head, 0, 1).reshape(seq_len, QH * HEAD)
    middle = (residual.astype(jnp.float32) + jnp.dot(attended, out_weight, preferred_element_type=jnp.float32)).astype(jnp.bfloat16)
    middle_f = middle.astype(jnp.float32)
    normed = (middle_f * lax.rsqrt(lax.optimization_barrier(jnp.mean(middle_f * middle_f, -1, keepdims=True)) + norm_epsilon) * norm_gain).astype(jnp.bfloat16)
    flattened = expert_ids.reshape(-1).astype(jnp.int32)
    most_rows = N_SP * N_TP * CAP
    slice_width = FFE // N_TP

    def one_expert(expert_index):
        matches = flattened == expert_index
        located = jnp.nonzero(matches, size=most_rows, fill_value=0)[0].astype(jnp.int32)
        is_live = jnp.arange(most_rows) < jnp.sum(matches.astype(jnp.int32))
        rows_in = normed[located // 2]
        gate_val = jnp.dot(rows_in, gate_proj[expert_index], preferred_element_type=jnp.float32)
        up_val = jnp.dot(rows_in, up_proj[expert_index], preferred_element_type=jnp.float32)
        hidden = lax.optimization_barrier((jax.nn.silu(gate_val) * up_val).astype(jnp.bfloat16)).astype(jnp.float32)
        down_slices = down_proj[expert_index].astype(jnp.float32).reshape(N_TP, slice_width, -1)
        slice_out = jnp.einsum('rsf,sfd->srd', hidden.reshape(most_rows, N_TP, slice_width), down_slices)
        slice_out = lax.optimization_barrier(slice_out.astype(jnp.bfloat16)).astype(jnp.float32)
        summed = lax.optimization_barrier(jnp.sum(slice_out, 0))
        return (located, summed * is_live[:, None].astype(jnp.float32))
    all_located, all_outputs = lax.map(one_expert, jnp.arange(N_SP, dtype=jnp.int32))
    assigned = jnp.zeros((seq_len * 2, normed.shape[1]), jnp.float32).at[all_located.reshape(-1)].add(all_outputs.reshape(-1, normed.shape[1]))
    routed = lax.optimization_barrier(jnp.sum(assigned.reshape(seq_len, 2, -1) * route_weight[..., None], 1))
    return (middle_f + routed).astype(jnp.bfloat16)
```

```python
import jax
import jax.numpy as jnp
from jax import lax
from jax.sharding import PartitionSpec as P

HEAD = 64
WINDOW = 128


norm_epsilon = 1e-06


SP = ("zg", "zl", "core")
TP = ("y", "xh", "xl")
SIZES = (4, 4, 2, 4, 2, 2)
ROUTE = ("zg", "zl", "core", "xl")
TEAM = ("y", "xh")


def from_behind(block, axis, distance):
    devices = range(lax.axis_size(axis))
    route = [(i - distance, i) for i in devices if i - distance in devices]
    return lax.ppermute(block, axis, route)


def exchange(blocks, axis):
    return lax.all_to_all(blocks, axis, 0, 0, tiled=True)


def sum_at_owner(array, axis):
    size = lax.axis_size(axis)
    pieces = exchange(array.reshape(size, -1, array.shape[-1]), axis)
    return jnp.sum(pieces.astype(jnp.float32), axis=0)


def to_team(weight):
    return lax.ppermute(weight, ("core", "xl"), [(0, 0), (1, 2), (2, 1), (3, 3)])


def across(block):
    return lax.ppermute(block, "core", [(0, 1), (1, 0)])


def rotary(values_in, positions, head_count):
    halfway = HEAD // 2
    frequency = 10000.0 ** (-jnp.arange(halfway, dtype=jnp.float32) * 2.0 / HEAD)
    angles = positions.astype(jnp.float32)[:, None] * frequency[None, :]
    cosine = jnp.cos(angles)[:, None, :]
    sine_part = jnp.sin(angles)[:, None, :]
    reshaped = values_in.astype(jnp.float32).reshape(values_in.shape[0], head_count, HEAD)
    front_part = reshaped[..., :halfway]
    back_part = reshaped[..., halfway:]
    turned = jnp.concatenate(
        [front_part * cosine - back_part * sine_part, back_part * cosine + front_part * sine_part],
        -1,
    )
    return turned.astype(jnp.bfloat16)


def attend(query_blocks, key_pairs, value_pairs, sink_grid, key_start):
    block_count = query_blocks.shape[0]
    window_len = query_blocks.shape[1]
    scores = jnp.einsum(
        "bqkgd,bskd->bkgqs", query_blocks, key_pairs, preferred_element_type=jnp.float32
    ) * HEAD ** (-0.5)
    row_idx = jnp.arange(window_len)[:, None]
    col_idx = jnp.arange(2 * window_len)[None, :]
    distance = row_idx - col_idx + window_len
    key_pos = key_start + jnp.arange(block_count)[:, None, None] * window_len + col_idx[None]
    allowed = (distance >= 0)[None] & (distance < window_len)[None] & (key_pos >= 0)
    scores = jnp.where(allowed[:, None, None], scores, -jnp.inf)
    sink_full = sink_grid[None, :, :, None]
    highest = jnp.maximum(jnp.max(scores, -1), sink_full)
    exp_scores = jnp.exp(scores - highest[..., None])
    denominator = jnp.sum(exp_scores, -1) + jnp.exp(sink_full - highest)
    weighted = jnp.einsum(
        "bkgqs,bskd->bkgqd",
        exp_scores.astype(jnp.bfloat16),
        value_pairs,
        preferred_element_type=jnp.float32,
    )
    normalized = weighted / denominator[..., None]
    return (
        jnp.transpose(normalized, (0, 3, 1, 2, 4))
        .astype(jnp.bfloat16)
        .reshape(block_count * window_len, -1)
    )


def slots(ids):
    rows = ids.shape[0]
    earlier = (jnp.arange(rows)[:, None] > jnp.arange(rows)[None, :])[:, None, :, None]
    same = ids[:, :, None, None] == ids[None, None]
    rank = jnp.sum((same & earlier).astype(jnp.int32), (2, 3))
    return (ids // 2) * 4 + rank * 2 + ids % 2


def expert_part(rows_in, weights):
    total = 0.0
    for gate, up, down in weights:
        gate_val = jnp.dot(rows_in, gate, preferred_element_type=jnp.float32)
        up_val = jnp.dot(rows_in, up, preferred_element_type=jnp.float32)
        hidden = (jax.nn.silu(gate_val) * up_val).astype(jnp.bfloat16)
        total = total + jnp.dot(hidden, down, preferred_element_type=jnp.float32)
    return total.astype(jnp.bfloat16)


def per_device(
    queries,
    key_rows,
    values,
    sink_logits,
    residual,
    out_weight,
    norm_gain,
    expert_ids,
    route_weight,
    gate_proj,
    up_proj,
    down_proj,
):
    local_len = queries.shape[0]
    q_heads = sink_logits.shape[0]
    kv_heads = key_rows.shape[1] // HEAD
    group_size = q_heads // kv_heads
    window_len = WINDOW
    seq_start = lax.axis_index(SP) * local_len
    rim_pair = jnp.stack([key_rows[local_len - window_len :], values[local_len - window_len :]])
    rim_pair = from_behind(rim_pair, SP, 1)
    gate = to_team(gate_proj[0])
    key_ext = jnp.concatenate([rim_pair[0], key_rows], 0)
    val_ext = jnp.concatenate([rim_pair[1], values], 0)
    positions = seq_start + jnp.arange(local_len, dtype=jnp.int32)
    ext_positions = seq_start - window_len + jnp.arange(local_len + window_len, dtype=jnp.int32)
    rot_query = rotary(queries, positions, q_heads)
    rot_key = rotary(key_ext, ext_positions, kv_heads)
    block_count = local_len // window_len
    query_blocks = rot_query.reshape(block_count, window_len, kv_heads, group_size, HEAD)
    key_blocks = rot_key.reshape(block_count + 1, window_len, kv_heads, HEAD)
    value_blocks = val_ext.reshape(block_count + 1, window_len, kv_heads, HEAD)
    key_pairs = jnp.concatenate([key_blocks[:-1], key_blocks[1:]], 1)
    value_pairs = jnp.concatenate([value_blocks[:-1], value_blocks[1:]], 1)
    sink_grid = sink_logits.reshape(kv_heads, group_size)
    attended = attend(query_blocks, key_pairs, value_pairs, sink_grid, seq_start - window_len)
    tok_rows, width = residual.shape
    shares = jnp.dot(attended, out_weight, preferred_element_type=jnp.float32).astype(jnp.bfloat16)
    shares, up_proj, down_proj = lax.optimization_barrier((shares, up_proj, down_proj))
    projected = sum_at_owner(shares, TP)
    up = to_team(up_proj[0])
    down = to_team(down_proj[0])
    middle = (residual.astype(jnp.float32) + projected).astype(jnp.bfloat16)
    middle_f = middle.astype(jnp.float32)
    normed = (
        middle_f
        * lax.rsqrt(jnp.mean(middle_f * middle_f, -1, keepdims=True) + norm_epsilon)
        * norm_gain
    ).astype(jnp.bfloat16)

    routes = 64
    first = lax.axis_index(TP) * tok_rows
    own_ids = lax.dynamic_slice_in_dim(expert_ids, first, tok_rows, 0)
    own_weights = lax.dynamic_slice_in_dim(route_weight, first, tok_rows, 0)
    slot = slots(own_ids)
    chosen = jnp.arange(routes, dtype=jnp.int32)[:, None, None] == slot[None]
    outbound = jnp.dot(
        jnp.any(chosen, -1).astype(jnp.bfloat16), normed, preferred_element_type=jnp.float32
    ).astype(jnp.bfloat16)
    arrived = exchange(outbound.reshape(routes, 16, width // 16), ROUTE).reshape(routes, width)

    team = 8
    gathered = exchange(jnp.broadcast_to(arrived[None], (team, routes, width)), TEAM)
    mine = (gate, up, down)
    others = tuple(across(w) for w in mine)
    partial_out = expert_part(gathered.reshape(team * routes, width), (mine, others))
    summed = sum_at_owner(partial_out, TEAM).astype(jnp.bfloat16)
    returned = exchange(summed.reshape(routes, 16, width // 16), ROUTE).reshape(routes, width)

    routed = 0.0
    for k in range(2):
        picked = jnp.dot(
            (slot[:, k, None] == jnp.arange(routes, dtype=jnp.int32)).astype(jnp.bfloat16),
            returned,
            preferred_element_type=jnp.float32,
        )
        routed = routed + picked * own_weights[:, k, None]
    return (middle_f + routed).astype(jnp.bfloat16)


def solution(mesh):
    fine = jax.sharding.Mesh(mesh.devices.reshape(SIZES), SP + TP)
    return jax.shard_map(
        per_device,
        mesh=fine,
        in_specs=(
            P(SP, TP),
            P(SP, TP),
            P(SP, TP),
            P(TP),
            P(SP + TP, None),
            P(TP, None),
            P(),
            P(SP, None),
            P(SP, None),
            P(SP, None, TP),
            P(SP, None, TP),
            P(SP, TP, None),
        ),
        out_specs=P(SP + TP, None),
        check_vma=False,
    )
```

```python
import jax
import jax.numpy as jnp
from jax import lax
from jax.experimental import pallas as pl
from jax.experimental.pallas import tpu as pltpu
from jax.sharding import PartitionSpec as P


HEAD = 64
WINDOW = 128


norm_epsilon = 1e-06


SP = ("zg", "zl", "core")
TP = ("y", "xh", "xl")
SIZES = (4, 4, 2, 4, 2, 2)
ROUTE = ("zg", "zl", "core", "xl")
TEAM = ("y", "xh")


def from_behind(block, axis, distance):
    devices = range(lax.axis_size(axis))
    route = [(i - distance, i) for i in devices if i - distance in devices]
    return lax.ppermute(block, axis, route)


def exchange(blocks, axis):
    return lax.all_to_all(blocks, axis, 0, 0, tiled=True)


def sum_at_owner(array, axis):
    size = lax.axis_size(axis)
    pieces = exchange(array.reshape(size, -1, array.shape[-1]), axis)
    return jnp.sum(pieces.astype(jnp.float32), axis=0)


def turn(weight):
    return lax.ppermute(weight, ("core", "xl"), [(0, 2), (2, 3), (3, 1), (1, 0)])


def pass_on(weight):
    return lax.ppermute(weight, ("core", "xl"), [(0, 2), (3, 1)])


def rotary(values_in, positions, head_count):
    halfway = HEAD // 2
    frequency = 10000.0 ** (-jnp.arange(halfway, dtype=jnp.float32) * 2.0 / HEAD)
    angles = positions.astype(jnp.float32)[:, None] * frequency[None, :]
    cosine = jnp.cos(angles)[:, None, :]
    sine_part = jnp.sin(angles)[:, None, :]
    reshaped = values_in.astype(jnp.float32).reshape(values_in.shape[0], head_count, HEAD)
    front_part = reshaped[..., :halfway]
    back_part = reshaped[..., halfway:]
    turned = jnp.concatenate(
        [front_part * cosine - back_part * sine_part, back_part * cosine + front_part * sine_part],
        -1,
    )
    return turned.astype(jnp.bfloat16)


def attend(query_blocks, key_pairs, value_pairs, sink_grid, key_start):
    block_count = query_blocks.shape[0]
    window_len = query_blocks.shape[1]
    scores = jnp.einsum(
        "bqkgd,bskd->bkgqs", query_blocks, key_pairs, preferred_element_type=jnp.float32
    ) * HEAD ** (-0.5)
    row_idx = jnp.arange(window_len)[:, None]
    col_idx = jnp.arange(2 * window_len)[None, :]
    distance = row_idx - col_idx + window_len
    key_pos = key_start + jnp.arange(block_count)[:, None, None] * window_len + col_idx[None]
    allowed = (distance >= 0)[None] & (distance < window_len)[None] & (key_pos >= 0)
    scores = jnp.where(allowed[:, None, None], scores, -jnp.inf)
    sink_full = sink_grid[None, :, :, None]
    highest = jnp.maximum(jnp.max(scores, -1), sink_full)
    exp_scores = jnp.exp(scores - highest[..., None])
    denominator = jnp.sum(exp_scores, -1) + jnp.exp(sink_full - highest)
    weighted = jnp.einsum(
        "bkgqs,bskd->bkgqd",
        exp_scores.astype(jnp.bfloat16),
        value_pairs,
        preferred_element_type=jnp.float32,
    )
    normalized = weighted / denominator[..., None]
    return (
        jnp.transpose(normalized, (0, 3, 1, 2, 4))
        .astype(jnp.bfloat16)
        .reshape(block_count * window_len, -1)
    )


IN_VMEM = pl.BlockSpec(memory_space=pltpu.VMEM)


def plan_kernel(ids_ref, ids_row_ref, spread_ref, collect_ref):
    rows, picks = ids_ref.shape
    routes = spread_ref.shape[0]
    down = lax.broadcasted_iota(jnp.int32, (rows, rows), 0)
    right = lax.broadcasted_iota(jnp.int32, (rows, rows), 1)
    spread = jnp.zeros((routes, rows), jnp.float32)
    for k in range(picks):
        col, row = ids_ref[:, k : k + 1], ids_row_ref[k : k + 1, :]
        rank_col = jnp.zeros((rows, 1), jnp.int32)
        rank_row = jnp.zeros((1, rows), jnp.int32)
        for j in range(picks):
            other_col, other_row = ids_ref[:, j : j + 1], ids_row_ref[j : j + 1, :]
            before = jnp.where((col == other_row) & (right < down), 1, 0)
            rank_col = rank_col + jnp.sum(before, 1, keepdims=True)
            before = jnp.where((other_col == row) & (down < right), 1, 0)
            rank_row = rank_row + jnp.sum(before, 0, keepdims=True)
        slot_col = (col >> 1) * 4 + rank_col * 2 + (col & 1)
        slot_row = (row >> 1) * 4 + rank_row * 2 + (row & 1)
        collect_ref[k * rows : (k + 1) * rows, :] = jnp.where(
            lax.broadcasted_iota(jnp.int32, (rows, routes), 1) == slot_col, 1.0, 0.0
        ).astype(jnp.bfloat16)
        spread = spread + jnp.where(
            lax.broadcasted_iota(jnp.int32, (routes, rows), 0) == slot_row, 1.0, 0.0
        )
    spread_ref[...] = spread.astype(jnp.bfloat16)


def plan(ids, routes):
    rows, picks = ids.shape
    return pl.pallas_call(
        plan_kernel,
        out_shape=(
            jax.ShapeDtypeStruct((routes, rows), jnp.bfloat16),
            jax.ShapeDtypeStruct((picks * rows, routes), jnp.bfloat16),
        ),
        in_specs=[IN_VMEM] * 2,
        out_specs=[IN_VMEM] * 2,
        cost_estimate=pl.CostEstimate(flops=10**6, bytes_accessed=8192, transcendentals=0),
    )(ids, ids.T)


def hold_kernel(in_ref, out_ref):
    out_ref[...] = in_ref[...]


def hold(array):
    return pl.pallas_call(
        hold_kernel,
        out_shape=jax.ShapeDtypeStruct(array.shape, array.dtype),
        in_specs=[IN_VMEM],
        out_specs=IN_VMEM,
        cost_estimate=pl.CostEstimate(flops=10**6, bytes_accessed=8192, transcendentals=0),
    )(array)


def expert_kernel(rows_ref, *refs):
    *weights, out_ref = refs
    rows = rows_ref[...]
    parts = []
    for gate, up, down in zip(*[iter(weights)] * 3, strict=True):
        gate_val = jnp.dot(rows, gate[...], preferred_element_type=jnp.float32)
        up_val = jnp.dot(rows, up[...], preferred_element_type=jnp.float32)
        hidden = gate_val / (1.0 + jnp.exp(-gate_val)) * up_val
        parts.append((hidden.astype(jnp.bfloat16), down))
    chunk = 512
    for at in range(0, out_ref.shape[1], chunk):
        total = jnp.zeros((rows.shape[0], chunk), jnp.float32)
        for hidden, down in parts:
            total += jnp.dot(
                hidden, down[:, at : at + chunk], preferred_element_type=jnp.float32
            )
        out_ref[:, at : at + chunk] = total.astype(jnp.bfloat16)


def expert_part(rows, *weights):
    count, width = rows.shape
    units = sum(w.shape[1] for w in weights[::3])
    return pl.pallas_call(
        expert_kernel,
        out_shape=jax.ShapeDtypeStruct((count, width), jnp.bfloat16),
        in_specs=[IN_VMEM] * (1 + len(weights)),
        out_specs=IN_VMEM,
        compiler_params=pltpu.CompilerParams(vmem_limit_bytes=40 * 2**20),
        cost_estimate=pl.CostEstimate(
            flops=6 * count * units * width,
            bytes_accessed=4 * count * width + 6 * units * width,
            transcendentals=count * units,
        ),
    )(rows, *weights)


def per_device(
    queries,
    key_rows,
    values,
    sink_logits,
    residual,
    out_weight,
    norm_gain,
    expert_ids,
    route_weight,
    gate_proj,
    up_proj,
    down_proj,
):
    local_len = queries.shape[0]
    q_heads = sink_logits.shape[0]
    kv_heads = key_rows.shape[1] // HEAD
    group_size = q_heads // kv_heads
    window_len = WINDOW
    seq_start = lax.axis_index(SP) * local_len
    rim_pair = jnp.stack([key_rows[local_len - window_len :], values[local_len - window_len :]])
    rim_pair = from_behind(rim_pair, SP, 1)
    own = (gate_proj[0], up_proj[0], down_proj[0])
    gate = turn(own[0])
    key_ext = jnp.concatenate([rim_pair[0], key_rows], 0)
    val_ext = jnp.concatenate([rim_pair[1], values], 0)
    positions = seq_start + jnp.arange(local_len, dtype=jnp.int32)
    ext_positions = seq_start - window_len + jnp.arange(local_len + window_len, dtype=jnp.int32)
    rot_query = rotary(queries, positions, q_heads)
    rot_key = rotary(key_ext, ext_positions, kv_heads)
    block_count = local_len // window_len
    query_blocks = rot_query.reshape(block_count, window_len, kv_heads, group_size, HEAD)
    key_blocks = rot_key.reshape(block_count + 1, window_len, kv_heads, HEAD)
    value_blocks = val_ext.reshape(block_count + 1, window_len, kv_heads, HEAD)
    key_pairs = jnp.concatenate([key_blocks[:-1], key_blocks[1:]], 1)
    value_pairs = jnp.concatenate([value_blocks[:-1], value_blocks[1:]], 1)
    sink_grid = sink_logits.reshape(kv_heads, group_size)
    attended = attend(query_blocks, key_pairs, value_pairs, sink_grid, seq_start - window_len)
    tok_rows, width = residual.shape
    first = lax.axis_index(TP) * tok_rows
    own_ids = lax.dynamic_slice_in_dim(expert_ids, first, tok_rows, 0)
    own_weights = lax.dynamic_slice_in_dim(route_weight, first, tok_rows, 0)
    shares = jnp.dot(attended, out_weight, preferred_element_type=jnp.float32).astype(jnp.bfloat16)
    projected = sum_at_owner(shares, TP)
    up = turn(own[1])
    down = turn(own[2])
    routes = 64
    spread, collect = plan(own_ids, routes)
    middle = (residual.astype(jnp.float32) + projected).astype(jnp.bfloat16)
    middle_f = middle.astype(jnp.float32)
    normed = (
        middle_f
        * lax.rsqrt(jnp.mean(middle_f * middle_f, -1, keepdims=True) + norm_epsilon)
        * norm_gain
    ).astype(jnp.bfloat16)

    outbound = jnp.dot(spread, normed, preferred_element_type=jnp.float32).astype(jnp.bfloat16)
    arrived = exchange(outbound.reshape(routes, 16, width // 16), ROUTE).reshape(routes, width)
    gate_too = pass_on(gate)
    up_too = pass_on(up)
    own_weights = hold(own_weights)

    team = 8
    spread_out = jnp.broadcast_to(arrived[None], (team, routes, width))
    gathered = exchange(spread_out, TEAM)
    down_too = pass_on(down)
    kept = lax.axis_index("core") == lax.axis_index("xl")
    second = [
        jnp.where(kept, mine, passed)
        for mine, passed in zip(own, (gate_too, up_too, down_too), strict=True)
    ]
    partial_out = expert_part(
        gathered.reshape(team * routes, width), gate, up, down, *second
    )
    summed = sum_at_owner(partial_out, TEAM).astype(jnp.bfloat16)
    returned = exchange(summed.reshape(routes, 16, width // 16), ROUTE).reshape(routes, width)

    picked = jnp.dot(collect, returned, preferred_element_type=jnp.float32)
    picked = picked.reshape(2, tok_rows, width)
    routed = picked[0] * own_weights[:, :1] + picked[1] * own_weights[:, 1:]
    return (middle_f + routed).astype(jnp.bfloat16)


def solution(mesh):
    fine = jax.sharding.Mesh(mesh.devices.reshape(SIZES), SP + TP)
    return jax.shard_map(
        per_device,
        mesh=fine,
        in_specs=(
            P(SP, TP),
            P(SP, TP),
            P(SP, TP),
            P(TP),
            P(SP + TP, None),
            P(TP, None),
            P(),
            P(SP, None),
            P(SP, None),
            P(SP, None, TP),
            P(SP, None, TP),
            P(SP, TP, None),
        ),
        out_specs=P(SP + TP, None),
        check_vma=False,
    )
```

```python
import jax
import jax.numpy as jnp
from jax import lax
from jax.experimental import pallas as pl
from jax.experimental.pallas import tpu as pltpu
from jax.sharding import PartitionSpec as P


HEAD = 64
WINDOW = 128


norm_epsilon = 1e-06


SP = ("zg", "zl", "core")
TP = ("y", "xh", "xl")
SIZES = (4, 4, 2, 4, 2, 2)
ROUTE = ("zg", "zl")


def from_behind(block, axis, distance):
    devices = range(lax.axis_size(axis))
    route = [(i - distance, i) for i in devices if i - distance in devices]
    return lax.ppermute(block, axis, route)


def exchange(blocks, axis):
    return lax.all_to_all(blocks, axis, 0, 0, tiled=True)


def turn(pack, side):
    columns = 4
    route = []
    for x in range(columns):
        here = x % 2
        beside = (x + side * (1 - 2 * here)) % columns
        route += [
            (here * columns + x, (1 - here) * columns + x),
            ((1 - here) * columns + x, (1 - here) * columns + beside),
        ]
    return lax.ppermute(pack, ("core", "xh", "xl"), route)


def pass_on(pack):
    return lax.ppermute(pack, ("core", "xl"), [(0, 2), (3, 1)])


IN_VMEM = pl.BlockSpec(memory_space=pltpu.VMEM)
IN_SMEM = pl.BlockSpec(memory_space=pltpu.SMEM)
IN_HBM = pl.BlockSpec(memory_space=pltpu.HBM)

LINES = 8
SLOTS = 4
PLANES = 16
PAIR = 2
RANKS = 2
DEPTH = 4


def near(array):
    return pltpu.with_memory_space_constraint(array, pltpu.VMEM)


def iota(shape, dim):
    return lax.broadcasted_iota(jnp.int32, shape, dim)


def one_hot(mask):
    return jnp.where(mask, 1.0, 0.0).astype(jnp.bfloat16)


def dot(left, right):
    return jnp.dot(left, right, preferred_element_type=jnp.float32)


def room(mib):
    return pltpu.CompilerParams(vmem_limit_bytes=mib * 2**20)


def price(flops, nbytes):
    return pl.CostEstimate(flops=flops, bytes_accessed=nbytes, transcendentals=0)


def turned(array, cosine, sine):
    half = HEAD // 2
    front, back = array[:half], array[half:]
    return jnp.concatenate(
        [front * cosine - back * sine, back * cosine + front * sine], 0
    ).astype(jnp.bfloat16)


def over_rows(left, right):
    return lax.dot_general(left, right, (((0,), (0,)), ((), ())), preferred_element_type=jnp.float32)


def attend_kernel(
    edge_ref, sink_ref, query_ref, key_ref, value_ref, rim_ref, *refs
):
    count = query_ref.shape[0]
    cosine_ref, sine_ref, weight_ref, out_ref = refs
    cosine, sine = cosine_ref[...], sine_ref[...]
    keys = jnp.concatenate([rim_ref[:HEAD], key_ref[...]], 1).astype(jnp.float32)
    keys = turned(keys, cosine, sine)
    values = jnp.concatenate([rim_ref[HEAD:], value_ref[...]], 1)
    queries = query_ref[...].astype(jnp.float32).T
    cosine, sine = cosine[:, WINDOW:], sine[:, WINDOW:]
    queries = [turned(queries[at : at + HEAD], cosine, sine) for at in (0, HEAD)]
    shape = (2 * WINDOW, 2 * WINDOW)
    key_at = lax.broadcasted_iota(jnp.int32, shape, 0)
    query_at = lax.broadcasted_iota(jnp.int32, shape, 1) & (WINDOW - 1)
    seen = (key_at > query_at) & (key_at <= query_at + WINDOW)
    first_head = lax.broadcasted_iota(jnp.int32, (1, 2 * WINDOW), 1) < WINDOW
    sink = jnp.where(first_head, sink_ref[0], sink_ref[1])
    for at in range(0, count, WINDOW):
        here = jnp.concatenate([q[:, at : at + WINDOW] for q in queries], 1)
        scores = over_rows(keys[:, at : at + 2 * WINDOW], here) * HEAD ** (-0.5)
        allowed = seen
        if at == 0:
            allowed = allowed & (key_at >= edge_ref[0])
        scores = jnp.where(allowed, scores, -jnp.inf)
        highest = jnp.maximum(jnp.max(scores, 0, keepdims=True), sink)
        raised = jnp.exp(scores - highest)
        denominator = jnp.sum(raised, 0, keepdims=True) + jnp.exp(sink - highest)
        weighted = jnp.dot(
            values[:, at : at + 2 * WINDOW],
            raised.astype(jnp.bfloat16),
            preferred_element_type=jnp.float32,
        )
        attended = (weighted / denominator).astype(jnp.bfloat16)
        attended = jnp.concatenate([attended[:, :WINDOW], attended[:, WINDOW:]], 0)
        out_ref[at : at + WINDOW] = over_rows(attended, weight_ref[...]).astype(jnp.bfloat16)


def attention_share(edge, sinks, queries, keys_t, values_t, rim, angles, weight):
    count, width = queries.shape[0], weight.shape[1]
    return pl.pallas_call(
        attend_kernel,
        out_shape=jax.ShapeDtypeStruct((count, width), jnp.bfloat16),
        in_specs=[IN_SMEM] * 2 + [IN_VMEM] * 7,
        out_specs=IN_VMEM,
        cost_estimate=pl.CostEstimate(
            flops=2 * count * 128 * (width + 1024),
            bytes_accessed=2 * (count + 128) * width,
            transcendentals=2 * count * 256,
        ),
    )(edge, sinks, queries, keys_t, values_t, *map(near, (rim, *angles)), weight)


def plan_kernel(ids_ref, ids_row_ref, spread_ref, collect_ref):
    rows, picks = ids_ref.shape
    lines = collect_ref.shape[2]
    below, right = iota((rows, rows), 0), iota((rows, rows), 1)
    spread = [jnp.zeros((lines, rows), jnp.float32)] * 2
    for k in range(picks):
        col, row = ids_ref[:, k : k + 1], ids_row_ref[k : k + 1, :]
        rank_col = jnp.zeros((rows, 1), jnp.int32)
        rank_row = jnp.zeros((1, rows), jnp.int32)
        for j in range(picks):
            other_col, other_row = ids_ref[:, j : j + 1], ids_row_ref[j : j + 1, :]
            before = jnp.where((col == other_row) & (right < below), 1, 0)
            rank_col = rank_col + jnp.sum(before, 1, keepdims=True)
            before = jnp.where((other_col == row) & (below < right), 1, 0)
            rank_row = rank_row + jnp.sum(before, 0, keepdims=True)
        for half in range(2):
            line_col = (col >> 1) * LINES + half * SLOTS + (col & 1) * RANKS + rank_col
            line_row = (row >> 1) * LINES + half * SLOTS + (row & 1) * RANKS + rank_row
            collect_ref[half, k * rows : (k + 1) * rows, :] = one_hot(
                iota((rows, lines), 1) == line_col
            )
            spread[half] = spread[half] + jnp.where(
                iota((lines, rows), 0) == line_row, 1.0, 0.0
            )
    for half in range(2):
        spread_ref[half] = spread[half].astype(jnp.bfloat16)


def plan(ids):
    rows, picks = ids.shape
    lines = PLANES * LINES
    return pl.pallas_call(
        plan_kernel,
        out_shape=(
            jax.ShapeDtypeStruct((2, lines, rows), jnp.bfloat16),
            jax.ShapeDtypeStruct((2, picks * rows, lines), jnp.bfloat16),
        ),
        in_specs=[IN_VMEM] * 2,
        out_specs=[IN_VMEM] * 2,
        compiler_params=room(16),
        cost_estimate=price(10**6, 2**14),
    )(ids, ids.T)


def pack_kernel(gate_ref, up_ref, down_ref, *refs):
    *out_refs, sems = refs
    copies = []
    for half, out_ref in enumerate(out_refs):
        lanes = pl.ds(half * 128, 128)
        pieces = [
            (gate_ref.at[:, :, lanes], out_ref.at[0]),
            (up_ref.at[:, :, lanes], out_ref.at[1]),
        ]
        for j in range(out_ref.shape[1]):
            pieces.append((down_ref.at[lanes, pl.ds(j * 128, 128)], out_ref.at[2, j]))
        for k, (source, target) in enumerate(pieces):
            copies.append(pltpu.make_async_copy(source, target, sems.at[half, k]))
    for copy in copies:
        copy.start()
    for copy in copies:
        copy.wait()


def pack(gate, up, down):
    units, width = down.shape
    blocks = width // 128
    shape = jax.ShapeDtypeStruct((3, blocks, 128, units // 2), jnp.bfloat16)
    return pl.pallas_call(
        pack_kernel,
        out_shape=(shape, shape),
        in_specs=[IN_HBM] * 3,
        out_specs=[IN_VMEM] * 2,
        scratch_shapes=[pltpu.SemaphoreType.DMA((2, 2 + blocks))],
        compiler_params=room(16),
        cost_estimate=price(10**6, 12 * units * width),
    )(gate.reshape(blocks, 128, units), up.reshape(blocks, 128, units), down)


def hold_kernel(in_ref, out_ref):
    out_ref[...] = in_ref[...]


def hold(array):
    return pl.pallas_call(
        hold_kernel,
        out_shape=jax.ShapeDtypeStruct(array.shape, array.dtype),
        in_specs=[IN_VMEM],
        out_specs=IN_VMEM,
        compiler_params=room(4),
        cost_estimate=price(10**6, 2**13),
    )(array)


def settle_kernel(shares_ref, residual_ref, gain_ref, spread_ref, middle_ref, out_ref):
    projected = jnp.sum(shares_ref[...].astype(jnp.float32), 0)
    middle = (residual_ref[...].astype(jnp.float32) + projected).astype(jnp.bfloat16)
    middle_ref[...] = middle
    middle = middle.astype(jnp.float32)
    square = jnp.mean(middle * middle, -1, keepdims=True)
    normed = (middle * lax.rsqrt(square + norm_epsilon) * gain_ref[...]).astype(jnp.bfloat16)
    half = normed.shape[1] // 2
    lines = dot(spread_ref[0], normed[:, :half]) + dot(spread_ref[1], normed[:, half:])
    out_ref[...] = lines.astype(jnp.bfloat16)


def settle(shares, residual, gain, spread):
    rows, width = residual.shape
    lines = spread.shape[1]
    return pl.pallas_call(
        settle_kernel,
        out_shape=(
            jax.ShapeDtypeStruct((rows, width), jnp.bfloat16),
            jax.ShapeDtypeStruct((lines, width // 2), jnp.bfloat16),
        ),
        in_specs=[IN_VMEM] * 4,
        out_specs=[IN_VMEM] * 2,
        compiler_params=room(16),
        cost_estimate=price(2 * lines * rows * width, 2 * shares.size),
    )(near(shares), residual, gain, near(spread))


def lines_of(half):
    shape = (PAIR * PLANES * RANKS, PLANES * LINES)
    row = iota(shape, 0)
    per_expert = PLANES * RANKS
    plane, slot = (row % per_expert) // RANKS, row // per_expert * RANKS + row % RANKS
    return iota(shape, 1) == plane * LINES + half * SLOTS + slot


def fan_kernel(lines_ref, out_ref):
    half = lines_ref.shape[1]
    for h in range(2):
        rows = dot(one_hot(lines_of(h)), lines_ref[...]).astype(jnp.bfloat16)
        for to in range(out_ref.shape[0]):
            out_ref[to, :, h * half : (h + 1) * half] = rows


def fan(lines, team):
    rows, width = PAIR * PLANES * RANKS, 2 * lines.shape[1]
    return pl.pallas_call(
        fan_kernel,
        out_shape=pltpu.VMEM((team, rows, width), jnp.bfloat16),
        in_specs=[IN_VMEM],
        out_specs=IN_VMEM,
        compiler_params=room(16),
        cost_estimate=price(2 * rows * lines.size * 2, 2 * team * rows * width),
    )(near(lines))


def fold_kernel(parts_ref, out_ref):
    half = out_ref.shape[1]
    rows = jnp.sum(parts_ref[...].astype(jnp.float32), 0).astype(jnp.bfloat16)
    lines = 0.0
    for h in range(2):
        take = one_hot(lines_of(h))
        lines = lines + lax.dot_general(
            take,
            rows[:, h * half : (h + 1) * half],
            (((0,), (0,)), ((), ())),
            preferred_element_type=jnp.float32,
        )
    out_ref[...] = lines.astype(jnp.bfloat16)


def fold(parts):
    width = parts.shape[2]
    lines = PLANES * LINES
    return pl.pallas_call(
        fold_kernel,
        out_shape=jax.ShapeDtypeStruct((lines, width // 2), jnp.bfloat16),
        in_specs=[IN_VMEM],
        out_specs=IN_VMEM,
        compiler_params=room(24),
        cost_estimate=price(2 * lines * parts.shape[1] * width, 2 * parts.size),
    )(near(parts))


def finish_kernel(lines_ref, collect_ref, share_ref, middle_ref, out_ref):
    rows = middle_ref.shape[0]
    half = lines_ref.shape[1]
    for h in range(2):
        at = slice(h * half, (h + 1) * half)
        picked = dot(collect_ref[h], lines_ref[...])
        routed = picked[:rows] * share_ref[:, :1] + picked[rows:] * share_ref[:, 1:]
        out_ref[:, at] = (middle_ref[:, at].astype(jnp.float32) + routed).astype(jnp.bfloat16)


def finish(lines, collect, shares, middle):
    return pl.pallas_call(
        finish_kernel,
        out_shape=jax.ShapeDtypeStruct(middle.shape, middle.dtype),
        in_specs=[IN_VMEM] * 4,
        out_specs=IN_VMEM,
        compiler_params=room(16),
        cost_estimate=price(4 * collect.size * lines.shape[1], 4 * lines.size),
    )(*map(near, (lines, collect)), shares, near(middle))


def expert_kernel(kept_ref, rows_ref, *refs):
    own, turned, passed = refs[0:2], refs[2:4], refs[4:6]
    out_ref, *slots, sems = refs[6:]
    gates, ups, downs = slots
    kept = kept_ref[0] == 1
    halves = range(len(own))

    def copy(source, slot, kind, half):
        units = pl.ds(half * 128, 128)
        place = (slot, slice(None), units) if kind == 2 else (slot, slice(None), slice(None), units)
        target = slots[kind].at[place]
        return pltpu.make_async_copy(source[half].at[kind], target, sems.at[slot, kind, half])

    def fetch(slot, kind):
        if slot == 0:
            for half in halves:
                copy(turned, slot, kind, half).start()
            return

        @pl.when(kept)
        def _():
            for half in halves:
                copy(own, slot, kind, half).start()

        @pl.when(jnp.logical_not(kept))
        def _():
            for half in halves:
                copy(passed, slot, kind, half).start()

    order = [(0, 0), (0, 1), (1, 0), (1, 1), (0, 2), (1, 2)]

    def ready(at):
        for half in halves:
            copy(turned, *order[at], half).wait()
        if at + DEPTH < len(order):
            fetch(*order[at + DEPTH])

    for at in range(DEPTH):
        fetch(*order[at])
    rows = rows_ref[...]
    hidden = []
    for slot in range(2):
        ready(2 * slot)
        gate_val = dot(rows, gates[slot].reshape(rows.shape[1], -1))
        ready(2 * slot + 1)
        up_val = dot(rows, ups[slot].reshape(rows.shape[1], -1))
        hidden.append((gate_val / (1.0 + jnp.exp(-gate_val)) * up_val).astype(jnp.bfloat16))
    ready(4)
    ready(5)
    chunk = 512
    for at in range(0, out_ref.shape[1], chunk):
        total = 0.0
        for slot in range(2):
            blocks = [downs[slot, j] for j in range(at // 128, (at + chunk) // 128)]
            total = total + dot(hidden[slot], jnp.concatenate(blocks, 1))
        out_ref[:, at : at + chunk] = total.astype(jnp.bfloat16)


def expert_part(kept, rows, own, turned, passed):
    count, width = rows.shape
    _, blocks, lanes, half = own[0].shape
    return pl.pallas_call(
        expert_kernel,
        out_shape=pltpu.VMEM((count, width), jnp.bfloat16),
        in_specs=[IN_SMEM, IN_VMEM] + [IN_HBM] * 6,
        out_specs=IN_VMEM,
        scratch_shapes=[
            pltpu.VMEM((2, blocks, lanes, 2 * half), jnp.bfloat16),
            pltpu.VMEM((2, blocks, lanes, 2 * half), jnp.bfloat16),
            pltpu.VMEM((2, blocks, 2 * half, lanes), jnp.bfloat16),
            pltpu.SemaphoreType.DMA((2, 3, 2)),
        ],
        compiler_params=room(32),
        cost_estimate=pl.CostEstimate(
            flops=24 * count * half * width,
            bytes_accessed=4 * count * width + 24 * half * width,
            transcendentals=4 * count * half,
        ),
    )(kept, near(rows), *own, *turned, *passed)


def per_device(
    queries,
    key_rows,
    values,
    sink_logits,
    residual,
    out_weight,
    norm_gain,
    expert_ids,
    route_weight,
    gate_proj,
    up_proj,
    down_proj,
):
    local_len = queries.shape[0]
    span = lax.axis_index(SP)
    keys_t, values_t = key_rows.T, values.T
    rim = jnp.concatenate([keys_t[:, -WINDOW:], values_t[:, -WINDOW:]], 0)
    rim = from_behind(rim, SP, 1)
    half = HEAD // 2
    frequency = 10000.0 ** (-jnp.arange(half, dtype=jnp.float32) * 2.0 / HEAD)
    positions = span * local_len - WINDOW + jnp.arange(local_len + WINDOW, dtype=jnp.int32)
    angles = positions.astype(jnp.float32)[None, :] * frequency[:, None]
    angles = (jnp.cos(angles), jnp.sin(angles))
    edge = jnp.where(span == 0, WINDOW, 0).astype(jnp.int32).reshape(1)
    shares = attention_share(edge, sink_logits, queries, keys_t, values_t, rim, angles, out_weight)
    tok_rows, width = residual.shape
    first = lax.axis_index(TP) * tok_rows
    own_ids = lax.dynamic_slice_in_dim(expert_ids, first, tok_rows, 0)
    own_weights = lax.dynamic_slice_in_dim(route_weight, first, tok_rows, 0)
    shares = exchange(shares.reshape(lax.axis_size(TP), -1, width), TP)
    own = pack(gate_proj[0], up_proj[0], down_proj[0])
    right = turn(own[0], 1)
    left = turn(own[1], -1)
    spread, collect = plan(own_ids)
    middle, lines = settle(shares, residual, norm_gain.reshape(1, -1), spread)
    lines = exchange(lines.reshape(PLANES, LINES, width // 2), ROUTE)
    team = lax.axis_size(TP) // PAIR
    fanned = fan(lines.reshape(PLANES * LINES, width // 2), team)
    gathered = exchange(fanned.reshape(team * PAIR, -1, width), TP)
    right_too = pass_on(right)
    left_too = pass_on(left)
    kept = (lax.axis_index("core") == lax.axis_index("xl")).astype(jnp.int32).reshape(1)
    own_weights = hold(own_weights)
    parts = expert_part(
        kept, gathered.reshape(-1, width), own, (right, left), (right_too, left_too)
    )
    parts = exchange(parts.reshape(team * PAIR, -1, width), TP)
    lines = fold(parts.reshape(team, -1, width))
    lines = exchange(lines.reshape(PLANES, LINES, width // 2), ROUTE)
    return finish(lines.reshape(PLANES * LINES, width // 2), collect, own_weights, middle)


def solution(mesh):
    fine = jax.sharding.Mesh(mesh.devices.reshape(SIZES), SP + TP)
    return jax.shard_map(
        per_device,
        mesh=fine,
        in_specs=(
            P(SP, TP),
            P(SP, TP),
            P(SP, TP),
            P(TP),
            P(SP + TP, None),
            P(TP, None),
            P(),
            P(SP, None),
            P(SP, None),
            P(SP, None, TP),
            P(SP, None, TP),
            P(SP, TP, None),
        ),
        out_specs=P(SP + TP, None),
        check_vma=False,
    )
```

```python
import jax
import jax.numpy as jnp
from jax import lax
from jax.experimental import pallas as pl
from jax.experimental.pallas import tpu as pltpu
from jax.sharding import PartitionSpec as P


HEAD = 64
WINDOW = 128


norm_epsilon = 1e-06


SP = ("z3", "z2", "z1", "z0", "core")
TP = ("y1", "y0", "x1", "x0")
ROUTE = ("z3", "z2", "z1", "z0")
CHIPS = ("x1", "x0", "y1", "y0")
OWNERS = ("x1", "x0", "y1", "y0")


def place(index, axes, order):
    return sum(
        ((index >> (len(axes) - 1 - axes.index(name))) & 1) << (len(order) - 1 - at)
        for at, name in enumerate(order)
    )


def column_parity(block):
    return place(block, CHIPS, TP) % 2


def from_behind(block, axis, distance):
    devices = range(lax.axis_size(axis))
    route = [(i - distance, i) for i in devices if i - distance in devices]
    return lax.ppermute(block, axis, route)


def exchange(blocks, axis):
    return lax.all_to_all(blocks, axis, 0, 0, tiled=True)


def turn(pack, side):
    columns = 4
    route = []
    for x in range(columns):
        here = x % 2
        beside = (x + side * (1 - 2 * here)) % columns
        route += [
            (here * columns + x, (1 - here) * columns + x),
            ((1 - here) * columns + x, (1 - here) * columns + beside),
        ]
    return lax.ppermute(pack, ("core", "x1", "x0"), route)


def pass_on(pack):
    return lax.ppermute(pack, ("core", "x0"), [(0, 2), (3, 1)])


IN_VMEM = pl.BlockSpec(memory_space=pltpu.VMEM)
IN_SMEM = pl.BlockSpec(memory_space=pltpu.SMEM)
IN_HBM = pl.BlockSpec(memory_space=pltpu.HBM)

LINES = 8
SLOTS = 4
PLANES = 16
PAIR = 2
RANKS = 2


def near(array):
    return pltpu.with_memory_space_constraint(array, pltpu.VMEM)


def iota(shape, dim):
    return lax.broadcasted_iota(jnp.int32, shape, dim)


def one_hot(mask):
    return jnp.where(mask, 1.0, 0.0).astype(jnp.bfloat16)


def dot(left, right):
    return jnp.dot(left, right, preferred_element_type=jnp.float32)


def room(mib):
    return pltpu.CompilerParams(vmem_limit_bytes=mib * 2**20)


def price(flops, nbytes):
    return pl.CostEstimate(flops=flops, bytes_accessed=nbytes, transcendentals=0)


def turned(array, cosine, sine):
    half = HEAD // 2
    front, back = array[:half], array[half:]
    return jnp.concatenate(
        [front * cosine - back * sine, back * cosine + front * sine], 0
    ).astype(jnp.bfloat16)


def over_rows(left, right):
    return lax.dot_general(left, right, (((0,), (0,)), ((), ())), preferred_element_type=jnp.float32)


def attend_kernel(
    edge_ref, sink_ref, query_ref, key_ref, value_ref, rim_ref, *refs
):
    count = query_ref.shape[0]
    cosine_ref, sine_ref, weight_ref, out_ref = refs
    cosine, sine = cosine_ref[...], sine_ref[...]
    keys = jnp.concatenate([rim_ref[:HEAD], key_ref[...]], 1).astype(jnp.float32)
    keys = turned(keys, cosine, sine)
    values = jnp.concatenate([rim_ref[HEAD:], value_ref[...]], 1)
    queries = query_ref[...].astype(jnp.float32).T
    cosine, sine = cosine[:, WINDOW:], sine[:, WINDOW:]
    queries = [turned(queries[at : at + HEAD], cosine, sine) for at in (0, HEAD)]
    shape = (2 * WINDOW, 2 * WINDOW)
    key_at = lax.broadcasted_iota(jnp.int32, shape, 0)
    query_at = lax.broadcasted_iota(jnp.int32, shape, 1) & (WINDOW - 1)
    seen = (key_at > query_at) & (key_at <= query_at + WINDOW)
    first_head = lax.broadcasted_iota(jnp.int32, (1, 2 * WINDOW), 1) < WINDOW
    sink = jnp.where(first_head, sink_ref[0], sink_ref[1])
    for at in range(0, count, WINDOW):
        here = jnp.concatenate([q[:, at : at + WINDOW] for q in queries], 1)
        scores = over_rows(keys[:, at : at + 2 * WINDOW], here) * HEAD ** (-0.5)
        allowed = seen
        if at == 0:
            allowed = allowed & (key_at >= edge_ref[0])
        scores = jnp.where(allowed, scores, -jnp.inf)
        highest = jnp.maximum(jnp.max(scores, 0, keepdims=True), sink)
        raised = jnp.exp(scores - highest)
        denominator = jnp.sum(raised, 0, keepdims=True) + jnp.exp(sink - highest)
        weighted = jnp.dot(
            values[:, at : at + 2 * WINDOW],
            raised.astype(jnp.bfloat16),
            preferred_element_type=jnp.float32,
        )
        attended = (weighted / denominator).astype(jnp.bfloat16)
        attended = jnp.concatenate([attended[:, :WINDOW], attended[:, WINDOW:]], 0)
        share = over_rows(attended, weight_ref[...]).astype(jnp.bfloat16)
        rows = out_ref.shape[1]
        for k in range(WINDOW // rows):
            to = place(at // rows + k, TP, OWNERS)
            out_ref[to] = share[k * rows : (k + 1) * rows]


def attention_share(edge, sinks, queries, keys_t, values_t, rim, angles, weight, chips):
    count, width = queries.shape[0], weight.shape[1]
    return pl.pallas_call(
        attend_kernel,
        out_shape=jax.ShapeDtypeStruct((chips, count // chips, width), jnp.bfloat16),
        in_specs=[IN_SMEM] * 2 + [IN_VMEM] * 7,
        out_specs=IN_VMEM,
        cost_estimate=pl.CostEstimate(
            flops=2 * count * 128 * (width + 1024),
            bytes_accessed=2 * (count + 128) * width,
            transcendentals=2 * count * 256,
        ),
    )(edge, sinks, queries, keys_t, values_t, *map(near, (rim, *angles)), weight)


def plan_kernel(ids_ref, ids_row_ref, spread_ref, collect_ref):
    rows, picks = ids_ref.shape
    lines = collect_ref.shape[2]
    below, right = iota((rows, rows), 0), iota((rows, rows), 1)
    spread = [jnp.zeros((lines, rows), jnp.float32)] * 2
    for k in range(picks):
        col, row = ids_ref[:, k : k + 1], ids_row_ref[k : k + 1, :]
        rank_col = jnp.zeros((rows, 1), jnp.int32)
        rank_row = jnp.zeros((1, rows), jnp.int32)
        for j in range(picks):
            other_col, other_row = ids_ref[:, j : j + 1], ids_row_ref[j : j + 1, :]
            before = jnp.where((col == other_row) & (right < below), 1, 0)
            rank_col = rank_col + jnp.sum(before, 1, keepdims=True)
            before = jnp.where((other_col == row) & (below < right), 1, 0)
            rank_row = rank_row + jnp.sum(before, 0, keepdims=True)
        for half in range(2):
            line_col = place(col >> 1, SP[:-1], ROUTE) * LINES + half * SLOTS + (col & 1) * RANKS + rank_col
            line_row = place(row >> 1, SP[:-1], ROUTE) * LINES + half * SLOTS + (row & 1) * RANKS + rank_row
            collect_ref[half, k * rows : (k + 1) * rows, :] = one_hot(
                iota((rows, lines), 1) == line_col
            )
            spread[half] = spread[half] + jnp.where(
                iota((lines, rows), 0) == line_row, 1.0, 0.0
            )
    for half in range(2):
        spread_ref[half] = spread[half].astype(jnp.bfloat16)


def plan(ids):
    rows, picks = ids.shape
    lines = PLANES * LINES
    return pl.pallas_call(
        plan_kernel,
        out_shape=(
            jax.ShapeDtypeStruct((2, lines, rows), jnp.bfloat16),
            jax.ShapeDtypeStruct((2, picks * rows, lines), jnp.bfloat16),
        ),
        in_specs=[IN_VMEM] * 2,
        out_specs=[IN_VMEM] * 2,
        compiler_params=room(16),
        cost_estimate=price(10**6, 2**14),
    )(ids, ids.T)


def pack_kernel(gate_ref, up_ref, down_ref, *refs):
    *out_refs, sems = refs
    copies = []
    for half, out_ref in enumerate(out_refs):
        lanes = pl.ds(half * 128, 128)
        pieces = [
            (gate_ref.at[:, :, lanes], out_ref.at[0]),
            (up_ref.at[:, :, lanes], out_ref.at[1]),
        ]
        for j in range(out_ref.shape[1]):
            pieces.append((down_ref.at[lanes, pl.ds(j * 128, 128)], out_ref.at[2, j]))
        for k, (source, target) in enumerate(pieces):
            copies.append(pltpu.make_async_copy(source, target, sems.at[half, k]))
    for copy in copies:
        copy.start()
    for copy in copies:
        copy.wait()


def pack(gate, up, down):
    units, width = down.shape
    blocks = width // 128
    shape = jax.ShapeDtypeStruct((3, blocks, 128, units // 2), jnp.bfloat16)
    return pl.pallas_call(
        pack_kernel,
        out_shape=(shape, shape),
        in_specs=[IN_HBM] * 3,
        out_specs=[IN_VMEM] * 2,
        scratch_shapes=[pltpu.SemaphoreType.DMA((2, 2 + blocks))],
        compiler_params=room(16),
        cost_estimate=price(10**6, 12 * units * width),
    )(gate.reshape(blocks, 128, units), up.reshape(blocks, 128, units), down)


def hold_kernel(in_ref, out_ref):
    out_ref[...] = in_ref[...]


def hold(array):
    return pl.pallas_call(
        hold_kernel,
        out_shape=jax.ShapeDtypeStruct(array.shape, array.dtype),
        in_specs=[IN_VMEM],
        out_specs=IN_VMEM,
        compiler_params=room(4),
        cost_estimate=price(10**6, 2**13),
    )(array)


def settle_kernel(shares_ref, residual_ref, gain_ref, spread_ref, middle_ref, out_ref):
    projected = jnp.sum(shares_ref[...].astype(jnp.float32), 0)
    middle = (residual_ref[...].astype(jnp.float32) + projected).astype(jnp.bfloat16)
    middle_ref[...] = middle
    middle = middle.astype(jnp.float32)
    square = jnp.mean(middle * middle, -1, keepdims=True)
    normed = (middle * lax.rsqrt(square + norm_epsilon) * gain_ref[...]).astype(jnp.bfloat16)
    half = normed.shape[1] // 2
    lines = dot(spread_ref[0], normed[:, :half]) + dot(spread_ref[1], normed[:, half:])
    out_ref[...] = lines.astype(jnp.bfloat16)


def settle(shares, residual, gain, spread):
    rows, width = residual.shape
    lines = spread.shape[1]
    return pl.pallas_call(
        settle_kernel,
        out_shape=(
            jax.ShapeDtypeStruct((rows, width), jnp.bfloat16),
            jax.ShapeDtypeStruct((lines, width // 2), jnp.bfloat16),
        ),
        in_specs=[IN_VMEM] * 4,
        out_specs=[IN_VMEM] * 2,
        compiler_params=room(16),
        cost_estimate=price(2 * lines * rows * width, 2 * shares.size),
    )(near(shares), residual, gain, near(spread))


def lines_of(half):
    shape = (PAIR * PLANES * RANKS, PLANES * LINES)
    row = iota(shape, 0)
    per_expert = PLANES * RANKS
    plane, slot = (row % per_expert) // RANKS, row // per_expert * RANKS + row % RANKS
    return iota(shape, 1) == plane * LINES + half * SLOTS + slot


def fan_kernel(lines_ref, out_ref):
    half = lines_ref.shape[1]
    count = out_ref.shape[1]
    for h in range(2):
        rows = dot(one_hot(lines_of(h)), lines_ref[...]).astype(jnp.bfloat16)
        for to in range(out_ref.shape[0]):
            at = column_parity(to) * count
            out_ref[to, :, h * half : (h + 1) * half] = rows[at : at + count]


def fan(lines, chips):
    rows, width = PLANES * RANKS, 2 * lines.shape[1]
    return pl.pallas_call(
        fan_kernel,
        out_shape=pltpu.VMEM((chips, rows, width), jnp.bfloat16),
        in_specs=[IN_VMEM],
        out_specs=IN_VMEM,
        compiler_params=room(16),
        cost_estimate=price(8 * rows * lines.size, 2 * chips * rows * width),
    )(near(lines))


def fold_kernel(parts_ref, out_ref):
    half = out_ref.shape[1]
    lines = 0.0
    totals = [0.0] * PAIR
    for chip in range(parts_ref.shape[0]):
        expert = column_parity(chip)
        totals[expert] = totals[expert] + parts_ref[chip].astype(jnp.float32)
    rows = jnp.concatenate(totals, 0).astype(jnp.bfloat16)
    for h in range(2):
        lines = lines + over_rows(one_hot(lines_of(h)), rows[:, h * half : (h + 1) * half])
    out_ref[...] = lines.astype(jnp.bfloat16)


def fold(parts):
    width = parts.shape[-1]
    lines = PLANES * LINES
    return pl.pallas_call(
        fold_kernel,
        out_shape=jax.ShapeDtypeStruct((lines, width // 2), jnp.bfloat16),
        in_specs=[IN_VMEM],
        out_specs=IN_VMEM,
        compiler_params=room(24),
        cost_estimate=price(2 * lines * PAIR * parts.shape[1] * width, 2 * parts.size),
    )(near(parts))


def finish_kernel(lines_ref, collect_ref, share_ref, middle_ref, out_ref):
    rows = middle_ref.shape[0]
    half = lines_ref.shape[1]
    for h in range(2):
        at = slice(h * half, (h + 1) * half)
        picked = dot(collect_ref[h], lines_ref[...])
        routed = picked[:rows] * share_ref[:, :1] + picked[rows:] * share_ref[:, 1:]
        out_ref[:, at] = (middle_ref[:, at].astype(jnp.float32) + routed).astype(jnp.bfloat16)


def finish(lines, collect, shares, middle):
    return pl.pallas_call(
        finish_kernel,
        out_shape=jax.ShapeDtypeStruct(middle.shape, middle.dtype),
        in_specs=[IN_VMEM] * 4,
        out_specs=IN_VMEM,
        compiler_params=room(16),
        cost_estimate=price(4 * collect.size * lines.shape[1], 4 * lines.size),
    )(*map(near, (lines, collect)), shares, near(middle))


def expert_kernel(kept_ref, rows_ref, *refs):
    own, turned, passed = refs[0:2], refs[2:4], refs[4:6]
    out_ref, *slots, sems = refs[6:]
    gates, ups, downs = slots
    kept = kept_ref[0] == 1
    halves = range(len(own))

    def copy(source, slot, kind, half):
        units = pl.ds(half * 128, 128)
        place = (slot, slice(None), units) if kind == 2 else (slot, slice(None), slice(None), units)
        target = slots[kind].at[place]
        return pltpu.make_async_copy(source[half].at[kind], target, sems.at[slot, kind, half])

    def fetch(slot, kind):
        if slot == 0:
            for half in halves:
                copy(turned, slot, kind, half).start()
            return

        @pl.when(kept)
        def _():
            for half in halves:
                copy(own, slot, kind, half).start()

        @pl.when(jnp.logical_not(kept))
        def _():
            for half in halves:
                copy(passed, slot, kind, half).start()

    def ready(slot, kinds):
        for kind in kinds:
            for half in halves:
                copy(turned, slot, kind, half).wait()

    for slot, kind in ((0, 0), (0, 1), (1, 0), (1, 1), (0, 2), (1, 2)):
        fetch(slot, kind)
    rows = rows_ref[...]
    hidden = []
    for slot in range(2):
        ready(slot, (0, 1))
        gate_val = dot(rows, gates[slot].reshape(rows.shape[1], -1))
        up_val = dot(rows, ups[slot].reshape(rows.shape[1], -1))
        hidden.append((gate_val / (1.0 + jnp.exp(-gate_val)) * up_val).astype(jnp.bfloat16))
    ready(0, (2,))
    ready(1, (2,))
    chunk = 512
    for at in range(0, out_ref.shape[1], chunk):
        total = 0.0
        for slot in range(2):
            blocks = [downs[slot, j] for j in range(at // 128, (at + chunk) // 128)]
            total = total + dot(hidden[slot], jnp.concatenate(blocks, 1))
        out_ref[:, at : at + chunk] = total.astype(jnp.bfloat16)


def expert_part(kept, rows, own, turned, passed):
    count, width = rows.shape
    _, blocks, lanes, half = own[0].shape
    return pl.pallas_call(
        expert_kernel,
        out_shape=pltpu.VMEM((count, width), jnp.bfloat16),
        in_specs=[IN_SMEM, IN_VMEM] + [IN_HBM] * 6,
        out_specs=IN_VMEM,
        scratch_shapes=[
            pltpu.VMEM((2, blocks, lanes, 2 * half), jnp.bfloat16),
            pltpu.VMEM((2, blocks, lanes, 2 * half), jnp.bfloat16),
            pltpu.VMEM((2, blocks, 2 * half, lanes), jnp.bfloat16),
            pltpu.SemaphoreType.DMA((2, 3, 2)),
        ],
        compiler_params=room(32),
        cost_estimate=pl.CostEstimate(
            flops=24 * count * half * width,
            bytes_accessed=4 * count * width + 24 * half * width,
            transcendentals=4 * count * half,
        ),
    )(kept, near(rows), *own, *turned, *passed)


def per_device(
    queries,
    key_rows,
    values,
    sink_logits,
    residual,
    out_weight,
    norm_gain,
    expert_ids,
    route_weight,
    gate_proj,
    up_proj,
    down_proj,
):
    local_len = queries.shape[0]
    span = lax.axis_index(SP)
    chips = lax.axis_size(TP)
    keys_t, values_t = key_rows.T, values.T
    rim = jnp.concatenate([keys_t[:, -WINDOW:], values_t[:, -WINDOW:]], 0)
    rim = from_behind(rim, SP, 1)
    half = HEAD // 2
    frequency = 10000.0 ** (-jnp.arange(half, dtype=jnp.float32) * 2.0 / HEAD)
    positions = span * local_len - WINDOW + jnp.arange(local_len + WINDOW, dtype=jnp.int32)
    angles = positions.astype(jnp.float32)[None, :] * frequency[:, None]
    angles = (jnp.cos(angles), jnp.sin(angles))
    edge = jnp.where(span == 0, WINDOW, 0).astype(jnp.int32).reshape(1)
    shares = attention_share(
        edge, sink_logits, queries, keys_t, values_t, rim, angles, out_weight, chips
    )
    tok_rows, width = residual.shape
    first = lax.axis_index(TP) * tok_rows
    own_ids = lax.dynamic_slice_in_dim(expert_ids, first, tok_rows, 0)
    own_weights = lax.dynamic_slice_in_dim(route_weight, first, tok_rows, 0)
    shares = exchange(shares, OWNERS)
    own = pack(gate_proj[0], up_proj[0], down_proj[0])
    right = turn(own[0], 1)
    left = turn(own[1], -1)
    spread, collect = plan(own_ids)
    middle, lines = settle(shares, residual, norm_gain.reshape(1, -1), spread)
    lines = exchange(lines.reshape(PLANES, LINES, width // 2), ROUTE)
    fanned = fan(lines.reshape(PLANES * LINES, width // 2), chips)
    gathered = exchange(fanned, CHIPS)
    right_too = pass_on(right)
    left_too = pass_on(left)
    kept = (lax.axis_index("core") == lax.axis_index("x0")).astype(jnp.int32).reshape(1)
    own_weights = hold(own_weights)
    parts = expert_part(
        kept, gathered.reshape(-1, width), own, (right, left), (right_too, left_too)
    )
    parts = exchange(parts.reshape(chips, -1, width), CHIPS)
    lines = fold(parts)
    lines = exchange(lines.reshape(PLANES, LINES, width // 2), ROUTE)
    return finish(lines.reshape(PLANES * LINES, width // 2), collect, own_weights, middle)


def solution(mesh):
    fine = jax.sharding.Mesh(mesh.devices.reshape([2] * len(SP + TP)), SP + TP)
    return jax.shard_map(
        per_device,
        mesh=fine,
        in_specs=(
            P(SP, TP),
            P(SP, TP),
            P(SP, TP),
            P(TP),
            P(SP + TP, None),
            P(TP, None),
            P(),
            P(SP, None),
            P(SP, None),
            P(SP, None, TP),
            P(SP, None, TP),
            P(SP, TP, None),
        ),
        out_specs=P(SP + TP, None),
        check_vma=False,
    )
```

```python
import jax
import jax.numpy as jnp
from jax import lax
from jax.experimental import pallas as pl
from jax.experimental.pallas import tpu as pltpu
from jax.sharding import PartitionSpec as P


HEAD = 64
WINDOW = 128


norm_epsilon = 1e-06


SP = ("z", "core")
TP = ("y", "x")
SIZES = (16, 2, 4, 4)
HEIGHT, WIDTH = SIZES[2:]
COLUMNS = [y * WIDTH + x for x in range(WIDTH) for y in range(HEIGHT)]
ORDERS = (COLUMNS, COLUMNS[::-1])
GROUPS = [[core * HEIGHT * WIDTH + chip for chip in order] for core, order in enumerate(ORDERS)]


def column_parity(block, core):
    return ORDERS[core][block] % WIDTH % 2


def from_behind(block, axis, distance):
    devices = range(lax.axis_size(axis))
    route = [(i - distance, i) for i in devices if i - distance in devices]
    return lax.ppermute(block, axis, route)


def in_plane(blocks):
    return lax.all_to_all(
        blocks, ("core",) + TP, 0, 0, axis_index_groups=GROUPS, tiled=True
    )


def along_z(blocks):
    return lax.all_to_all(blocks, "z", 0, 0, tiled=True)


def turn(pack, side):
    columns = 4
    route = []
    for x in range(columns):
        here = x % 2
        beside = (x + side * (1 - 2 * here)) % columns
        route += [
            (here * columns + x, (1 - here) * columns + x),
            ((1 - here) * columns + x, (1 - here) * columns + beside),
        ]
    return lax.ppermute(pack, ("core", "x"), route)


def pass_on(pack):
    route = [((x % 2) * WIDTH + x, (1 - x % 2) * WIDTH + x) for x in range(WIDTH)]
    return lax.ppermute(pack, ("core", "x"), route)


IN_VMEM = pl.BlockSpec(memory_space=pltpu.VMEM)
IN_SMEM = pl.BlockSpec(memory_space=pltpu.SMEM)
IN_HBM = pl.BlockSpec(memory_space=pltpu.HBM)

LINES = 8
SLOTS = 4
PLANES = 16
PAIR = 2
RANKS = 2


def near(array):
    return pltpu.with_memory_space_constraint(array, pltpu.VMEM)


def far(array):
    return pltpu.with_memory_space_constraint(array, pltpu.HBM)


def iota(shape, dim):
    return lax.broadcasted_iota(jnp.int32, shape, dim)


def one_hot(mask):
    return jnp.where(mask, 1.0, 0.0).astype(jnp.bfloat16)


def dot(left, right):
    return jnp.dot(left, right, preferred_element_type=jnp.float32)


def room(mib):
    return pltpu.CompilerParams(vmem_limit_bytes=mib * 2**20)


def price(flops, nbytes):
    return pl.CostEstimate(flops=flops, bytes_accessed=nbytes, transcendentals=0)


def turned(array, cosine, sine):
    half = HEAD // 2
    front, back = array[:half], array[half:]
    return jnp.concatenate(
        [front * cosine - back * sine, back * cosine + front * sine], 0
    ).astype(jnp.bfloat16)


def over_rows(left, right):
    return lax.dot_general(left, right, (((0,), (0,)), ((), ())), preferred_element_type=jnp.float32)


def attend_kernel(
    core_ref, edge_ref, sink_ref, query_ref, key_ref, value_ref, rim_ref, *refs
):
    count = query_ref.shape[0]
    cosine_ref, sine_ref, weight_ref, out_ref = refs
    cosine, sine = cosine_ref[...], sine_ref[...]
    keys = jnp.concatenate([rim_ref[:HEAD], key_ref[...]], 1).astype(jnp.float32)
    keys = turned(keys, cosine, sine)
    values = jnp.concatenate([rim_ref[HEAD:], value_ref[...]], 1)
    queries = query_ref[...].astype(jnp.float32).T
    cosine, sine = cosine[:, WINDOW:], sine[:, WINDOW:]
    queries = [turned(queries[at : at + HEAD], cosine, sine) for at in (0, HEAD)]
    shape = (2 * WINDOW, 2 * WINDOW)
    key_at = lax.broadcasted_iota(jnp.int32, shape, 0)
    query_at = lax.broadcasted_iota(jnp.int32, shape, 1) & (WINDOW - 1)
    seen = (key_at > query_at) & (key_at <= query_at + WINDOW)
    first_head = lax.broadcasted_iota(jnp.int32, (1, 2 * WINDOW), 1) < WINDOW
    sink = jnp.where(first_head, sink_ref[0], sink_ref[1])
    for at in range(0, count, WINDOW):
        here = jnp.concatenate([q[:, at : at + WINDOW] for q in queries], 1)
        scores = over_rows(keys[:, at : at + 2 * WINDOW], here) * HEAD ** (-0.5)
        allowed = seen
        if at == 0:
            allowed = allowed & (key_at >= edge_ref[0])
        scores = jnp.where(allowed, scores, -jnp.inf)
        highest = jnp.maximum(jnp.max(scores, 0, keepdims=True), sink)
        raised = jnp.exp(scores - highest)
        denominator = jnp.sum(raised, 0, keepdims=True) + jnp.exp(sink - highest)
        weighted = jnp.dot(
            values[:, at : at + 2 * WINDOW],
            raised.astype(jnp.bfloat16),
            preferred_element_type=jnp.float32,
        )
        attended = (weighted / denominator).astype(jnp.bfloat16)
        attended = jnp.concatenate([attended[:, :WINDOW], attended[:, WINDOW:]], 0)
        share = over_rows(attended, weight_ref[...]).astype(jnp.bfloat16)
        rows = out_ref.shape[1]
        for k in range(WINDOW // rows):
            owner = at // rows + k
            to = jnp.where(core_ref[0] == 0, *(order.index(owner) for order in ORDERS))
            out_ref[to] = share[k * rows : (k + 1) * rows]


def attention_share(core, edge, sinks, queries, keys_t, values_t, rim, angles, weight, chips):
    count, width = queries.shape[0], weight.shape[1]
    return pl.pallas_call(
        attend_kernel,
        out_shape=jax.ShapeDtypeStruct((chips, count // chips, width), jnp.bfloat16),
        in_specs=[IN_SMEM] * 3 + [IN_VMEM] * 7,
        out_specs=IN_VMEM,
        cost_estimate=pl.CostEstimate(
            flops=2 * count * 128 * (width + 1024),
            bytes_accessed=2 * (count + 128) * width,
            transcendentals=2 * count * 256,
        ),
    )(core, edge, sinks, queries, keys_t, values_t, *map(near, (rim, *angles)), weight)


def rim_kernel(key_ref, value_ref, out_ref, sems):
    copies = [
        pltpu.make_async_copy(
            ref.at[:, pl.ds(ref.shape[1] - WINDOW, WINDOW)],
            out_ref.at[pl.ds(k * HEAD, HEAD)],
            sems.at[k],
        )
        for k, ref in enumerate((key_ref, value_ref))
    ]
    for copy in copies:
        copy.start()
    for copy in copies:
        copy.wait()


def rim_of(keys_t, values_t):
    return pl.pallas_call(
        rim_kernel,
        out_shape=pltpu.VMEM((2 * HEAD, WINDOW), keys_t.dtype),
        in_specs=[IN_HBM] * 2,
        out_specs=IN_VMEM,
        scratch_shapes=[pltpu.SemaphoreType.DMA((2,))],
        cost_estimate=price(10**5, 2**16),
    )(far(keys_t), far(values_t))


def plan_kernel(ids_ref, ids_row_ref, spread_ref, collect_ref):
    rows, picks = ids_ref.shape
    lines = collect_ref.shape[2]
    below, right = iota((rows, rows), 0), iota((rows, rows), 1)
    spread = [jnp.zeros((lines, rows), jnp.float32)] * 2
    for k in range(picks):
        col, row = ids_ref[:, k : k + 1], ids_row_ref[k : k + 1, :]
        rank_col = jnp.zeros((rows, 1), jnp.int32)
        rank_row = jnp.zeros((1, rows), jnp.int32)
        for j in range(picks):
            other_col, other_row = ids_ref[:, j : j + 1], ids_row_ref[j : j + 1, :]
            before = jnp.where((col == other_row) & (right < below), 1, 0)
            rank_col = rank_col + jnp.sum(before, 1, keepdims=True)
            before = jnp.where((other_col == row) & (below < right), 1, 0)
            rank_row = rank_row + jnp.sum(before, 0, keepdims=True)
        for half in range(2):
            line_col = (col >> 1) * LINES + half * SLOTS + (col & 1) * RANKS + rank_col
            line_row = (row >> 1) * LINES + half * SLOTS + (row & 1) * RANKS + rank_row
            collect_ref[half, k * rows : (k + 1) * rows, :] = one_hot(
                iota((rows, lines), 1) == line_col
            )
            spread[half] = spread[half] + jnp.where(
                iota((lines, rows), 0) == line_row, 1.0, 0.0
            )
    for half in range(2):
        spread_ref[half] = spread[half].astype(jnp.bfloat16)


def plan(ids):
    rows, picks = ids.shape
    lines = PLANES * LINES
    return pl.pallas_call(
        plan_kernel,
        out_shape=(
            jax.ShapeDtypeStruct((2, lines, rows), jnp.bfloat16),
            jax.ShapeDtypeStruct((2, picks * rows, lines), jnp.bfloat16),
        ),
        in_specs=[IN_VMEM] * 2,
        out_specs=[IN_VMEM] * 2,
        compiler_params=room(16),
        cost_estimate=price(10**6, 2**14),
    )(ids, ids.T)


def pack_kernel(gate_ref, up_ref, down_ref, *refs):
    *out_refs, sems = refs
    copies = []
    for half, out_ref in enumerate(out_refs):
        lanes = pl.ds(half * 128, 128)
        pieces = [
            (gate_ref.at[:, :, lanes], out_ref.at[0]),
            (up_ref.at[:, :, lanes], out_ref.at[1]),
        ]
        for j in range(out_ref.shape[1]):
            pieces.append((down_ref.at[lanes, pl.ds(j * 128, 128)], out_ref.at[2, j]))
        for k, (source, target) in enumerate(pieces):
            copies.append(pltpu.make_async_copy(source, target, sems.at[half, k]))
    for copy in copies:
        copy.start()
    for copy in copies:
        copy.wait()


def pack(gate, up, down):
    units, width = down.shape
    blocks = width // 128
    shape = jax.ShapeDtypeStruct((3, blocks, 128, units // 2), jnp.bfloat16)
    return pl.pallas_call(
        pack_kernel,
        out_shape=(shape, shape),
        in_specs=[IN_HBM] * 3,
        out_specs=[IN_VMEM] * 2,
        scratch_shapes=[pltpu.SemaphoreType.DMA((2, 2 + blocks))],
        cost_estimate=price(10**6, 12 * units * width),
    )(*map(far, (gate.reshape(blocks, 128, units), up.reshape(blocks, 128, units), down)))


def hold_kernel(in_ref, out_ref):
    out_ref[...] = in_ref[...]


def hold(array):
    return pl.pallas_call(
        hold_kernel,
        out_shape=jax.ShapeDtypeStruct(array.shape, array.dtype),
        in_specs=[IN_VMEM],
        out_specs=IN_VMEM,
        compiler_params=room(4),
        cost_estimate=price(10**6, 2**13),
    )(array)


def settle_kernel(shares_ref, residual_ref, gain_ref, spread_ref, middle_ref, out_ref):
    projected = jnp.sum(shares_ref[...].astype(jnp.float32), 0)
    middle = (residual_ref[...].astype(jnp.float32) + projected).astype(jnp.bfloat16)
    middle_ref[...] = middle
    middle = middle.astype(jnp.float32)
    square = jnp.mean(middle * middle, -1, keepdims=True)
    normed = (middle * lax.rsqrt(square + norm_epsilon) * gain_ref[...]).astype(jnp.bfloat16)
    half = normed.shape[1] // 2
    lines = dot(spread_ref[0], normed[:, :half]) + dot(spread_ref[1], normed[:, half:])
    out_ref[...] = lines.astype(jnp.bfloat16)


def settle(shares, residual, gain, spread):
    rows, width = residual.shape
    lines = spread.shape[1]
    return pl.pallas_call(
        settle_kernel,
        out_shape=(
            jax.ShapeDtypeStruct((rows, width), jnp.bfloat16),
            jax.ShapeDtypeStruct((lines, width // 2), jnp.bfloat16),
        ),
        in_specs=[IN_VMEM] * 4,
        out_specs=[IN_VMEM] * 2,
        compiler_params=room(16),
        cost_estimate=price(2 * lines * rows * width, 2 * shares.size),
    )(near(shares), residual, gain, near(spread))


def lines_of(half):
    shape = (PAIR * PLANES * RANKS, PLANES * LINES)
    row = iota(shape, 0)
    per_expert = PLANES * RANKS
    plane, slot = (row % per_expert) // RANKS, row // per_expert * RANKS + row % RANKS
    return iota(shape, 1) == plane * LINES + half * SLOTS + slot


def for_each_core(core_ref, body):
    for core in range(2):

        @pl.when(core_ref[0] == core)
        def _():
            body(core)


def fan_kernel(core_ref, lines_ref, out_ref):
    half = lines_ref.shape[1]
    count = out_ref.shape[1]
    for h in range(2):
        rows = dot(one_hot(lines_of(h)), lines_ref[...]).astype(jnp.bfloat16)

        def hand_out(core):
            for to in range(out_ref.shape[0]):
                at = column_parity(to, core) * count
                out_ref[to, :, h * half : (h + 1) * half] = rows[at : at + count]

        for_each_core(core_ref, hand_out)


def fan(core, lines, chips):
    rows, width = PLANES * RANKS, 2 * lines.shape[1]
    return pl.pallas_call(
        fan_kernel,
        out_shape=jax.ShapeDtypeStruct((chips, rows, width), jnp.bfloat16),
        in_specs=[IN_SMEM, IN_VMEM],
        out_specs=IN_VMEM,
        compiler_params=room(16),
        cost_estimate=price(8 * rows * lines.size, 2 * chips * rows * width),
    )(core, near(lines))


def fold_kernel(core_ref, parts_ref, out_ref, rows_ref):
    half = out_ref.shape[1]
    count = parts_ref.shape[1]

    def add_up(core):
        totals = [0.0] * PAIR
        for chip in range(parts_ref.shape[0]):
            expert = column_parity(chip, core)
            totals[expert] = totals[expert] + parts_ref[chip].astype(jnp.float32)
        for expert, total in enumerate(totals):
            rows_ref[expert * count : (expert + 1) * count] = total.astype(jnp.bfloat16)

    for_each_core(core_ref, add_up)
    lines = 0.0
    for h in range(2):
        lines = lines + over_rows(one_hot(lines_of(h)), rows_ref[:, h * half : (h + 1) * half])
    out_ref[...] = lines.astype(jnp.bfloat16)


def fold(core, parts):
    _, rows, width = parts.shape
    lines = PLANES * LINES
    return pl.pallas_call(
        fold_kernel,
        out_shape=jax.ShapeDtypeStruct((lines, width // 2), jnp.bfloat16),
        in_specs=[IN_SMEM, IN_VMEM],
        out_specs=IN_VMEM,
        scratch_shapes=[pltpu.VMEM((PAIR * rows, width), jnp.bfloat16)],
        compiler_params=room(24),
        cost_estimate=price(2 * lines * PAIR * rows * width, 2 * parts.size),
    )(core, near(parts))


def finish_kernel(lines_ref, collect_ref, share_ref, middle_ref, out_ref):
    rows = middle_ref.shape[0]
    half = lines_ref.shape[1]
    for h in range(2):
        at = slice(h * half, (h + 1) * half)
        picked = dot(collect_ref[h], lines_ref[...])
        routed = picked[:rows] * share_ref[:, :1] + picked[rows:] * share_ref[:, 1:]
        out_ref[:, at] = (middle_ref[:, at].astype(jnp.float32) + routed).astype(jnp.bfloat16)


def finish(lines, collect, shares, middle):
    return pl.pallas_call(
        finish_kernel,
        out_shape=jax.ShapeDtypeStruct(middle.shape, middle.dtype),
        in_specs=[IN_VMEM] * 4,
        out_specs=IN_VMEM,
        compiler_params=room(16),
        cost_estimate=price(4 * collect.size * lines.shape[1], 4 * lines.size),
    )(*map(near, (lines, collect)), shares, near(middle))


def expert_kernel(kept_ref, rows_ref, *refs):
    own, turned, passed = refs[0:2], refs[2:4], refs[4:6]
    out_ref, *slots, sems = refs[6:]
    gates, ups, downs = slots
    kept = kept_ref[0] == 1
    halves = range(len(own))

    def copy(source, slot, kind, half):
        units = pl.ds(half * 128, 128)
        place = (slot, slice(None), units) if kind == 2 else (slot, slice(None), slice(None), units)
        target = slots[kind].at[place]
        return pltpu.make_async_copy(source[half].at[kind], target, sems.at[slot, kind, half])

    def fetch(slot, kind):
        if slot == 0:
            for half in halves:
                copy(turned, slot, kind, half).start()
            return

        @pl.when(kept)
        def _():
            for half in halves:
                copy(own, slot, kind, half).start()

        @pl.when(jnp.logical_not(kept))
        def _():
            for half in halves:
                copy(passed, slot, kind, half).start()

    def ready(slot, kinds):
        for kind in kinds:
            for half in halves:
                copy(turned, slot, kind, half).wait()

    for slot, kind in ((0, 0), (0, 1), (1, 0), (1, 1), (0, 2), (1, 2)):
        fetch(slot, kind)
    rows = rows_ref[...]
    hidden = []
    for slot in range(2):
        ready(slot, (0, 1))
        gate_val = dot(rows, gates[slot].reshape(rows.shape[1], -1))
        up_val = dot(rows, ups[slot].reshape(rows.shape[1], -1))
        hidden.append((gate_val / (1.0 + jnp.exp(-gate_val)) * up_val).astype(jnp.bfloat16))
    ready(0, (2,))
    ready(1, (2,))
    chunk = 512
    for at in range(0, out_ref.shape[1], chunk):
        total = 0.0
        for slot in range(2):
            blocks = [downs[slot, j] for j in range(at // 128, (at + chunk) // 128)]
            total = total + dot(hidden[slot], jnp.concatenate(blocks, 1))
        out_ref[:, at : at + chunk] = total.astype(jnp.bfloat16)


def expert_part(kept, rows, own, turned, passed):
    count, width = rows.shape
    _, blocks, lanes, half = own[0].shape
    return pl.pallas_call(
        expert_kernel,
        out_shape=pltpu.VMEM((count, width), jnp.bfloat16),
        in_specs=[IN_SMEM, IN_VMEM] + [IN_HBM] * 6,
        out_specs=IN_VMEM,
        scratch_shapes=[
            pltpu.VMEM((2, blocks, lanes, 2 * half), jnp.bfloat16),
            pltpu.VMEM((2, blocks, lanes, 2 * half), jnp.bfloat16),
            pltpu.VMEM((2, blocks, 2 * half, lanes), jnp.bfloat16),
            pltpu.SemaphoreType.DMA((2, 3, 2)),
        ],
        compiler_params=room(32),
        cost_estimate=pl.CostEstimate(
            flops=24 * count * half * width,
            bytes_accessed=4 * count * width + 24 * half * width,
            transcendentals=4 * count * half,
        ),
    )(kept, near(rows), *map(far, (*own, *turned, *passed)))


def per_device(
    queries,
    key_rows,
    values,
    sink_logits,
    residual,
    out_weight,
    norm_gain,
    expert_ids,
    route_weight,
    gate_proj,
    up_proj,
    down_proj,
):
    local_len = queries.shape[0]
    span = lax.axis_index(SP)
    core = lax.axis_index("core")
    core_at = core.astype(jnp.int32).reshape(1)
    chips = lax.axis_size(TP)
    keys_t, values_t = key_rows.T, values.T
    rim = from_behind(rim_of(keys_t, values_t), SP, 1)
    half = HEAD // 2
    frequency = 10000.0 ** (-jnp.arange(half, dtype=jnp.float32) * 2.0 / HEAD)
    positions = span * local_len - WINDOW + jnp.arange(local_len + WINDOW, dtype=jnp.int32)
    angles = positions.astype(jnp.float32)[None, :] * frequency[:, None]
    angles = (jnp.cos(angles), jnp.sin(angles))
    edge = jnp.where(span == 0, WINDOW, 0).astype(jnp.int32).reshape(1)
    shares = attention_share(
        core_at, edge, sink_logits, queries, keys_t, values_t, rim, angles, out_weight, chips
    )
    tok_rows, width = residual.shape
    first = lax.axis_index(TP) * tok_rows
    own_ids = lax.dynamic_slice_in_dim(expert_ids, first, tok_rows, 0)
    own_weights = lax.dynamic_slice_in_dim(route_weight, first, tok_rows, 0)
    shares = in_plane(shares)
    own = pack(gate_proj[0], up_proj[0], down_proj[0])
    right = turn(own[0], 1)
    left = turn(own[1], -1)
    spread, collect = plan(own_ids)
    middle, lines = settle(shares, residual, norm_gain.reshape(1, -1), spread)
    lines = along_z(lines.reshape(PLANES, LINES, width // 2))
    fanned = fan(core_at, lines.reshape(PLANES * LINES, width // 2), chips)
    gathered = in_plane(fanned)
    right_too = pass_on(right)
    left_too = pass_on(left)
    kept = (core == lax.axis_index("x") % 2).astype(jnp.int32).reshape(1)
    own_weights = hold(own_weights)
    parts = expert_part(
        kept, gathered.reshape(-1, width), own, (right, left), (right_too, left_too)
    )
    parts = in_plane(parts.reshape(chips, -1, width))
    lines = fold(core_at, parts)
    lines = along_z(lines.reshape(PLANES, LINES, width // 2))
    return finish(lines.reshape(PLANES * LINES, width // 2), collect, own_weights, middle)


def solution(mesh):
    fine = jax.sharding.Mesh(mesh.devices.reshape(SIZES), SP + TP)
    return jax.shard_map(
        per_device,
        mesh=fine,
        in_specs=(
            P(SP, TP),
            P(SP, TP),
            P(SP, TP),
            P(TP),
            P(SP + TP, None),
            P(TP, None),
            P(),
            P(SP, None),
            P(SP, None),
            P(SP, None, TP),
            P(SP, None, TP),
            P(SP, TP, None),
        ),
        out_specs=P(SP + TP, None),
        check_vma=False,
    )
```

```python
import jax
import jax.numpy as jnp
from jax import lax
from jax.experimental import pallas as pl
from jax.experimental.pallas import tpu as pltpu
from jax.sharding import PartitionSpec as P


HEAD = 64
WINDOW = 128


norm_epsilon = 1e-06


SP = ("z", "core")
TP = ("y", "x")
SIZES = (16, 2, 4, 4)
HEIGHT, WIDTH = SIZES[2:]
COLUMNS = [y * WIDTH + x for x in range(WIDTH) for y in range(HEIGHT)]
ORDERS = (COLUMNS, COLUMNS[::-1])
GROUPS = [[core * HEIGHT * WIDTH + chip for chip in order] for core, order in enumerate(ORDERS)]


def column_parity(block, core):
    return ORDERS[core][block] % WIDTH % 2


def from_behind(block, axis, distance):
    devices = range(lax.axis_size(axis))
    route = [(i - distance, i) for i in devices if i - distance in devices]
    return lax.ppermute(block, axis, route)


def in_plane(blocks):
    return lax.all_to_all(
        blocks, ("core",) + TP, 0, 0, axis_index_groups=GROUPS, tiled=True
    )


def along_z(blocks):
    return lax.all_to_all(blocks, "z", 0, 0, tiled=True)


def turn(pack, side):
    columns = 4
    route = []
    for x in range(columns):
        here = x % 2
        beside = (x + side * (1 - 2 * here)) % columns
        route += [
            (here * columns + x, (1 - here) * columns + x),
            ((1 - here) * columns + x, (1 - here) * columns + beside),
        ]
    return lax.ppermute(pack, ("core", "x"), route)


def pass_on(pack):
    route = [((x % 2) * WIDTH + x, (1 - x % 2) * WIDTH + x) for x in range(WIDTH)]
    return lax.ppermute(pack, ("core", "x"), route)


IN_VMEM = pl.BlockSpec(memory_space=pltpu.VMEM)
IN_SMEM = pl.BlockSpec(memory_space=pltpu.SMEM)
IN_HBM = pl.BlockSpec(memory_space=pltpu.HBM)

LINES = 8
SLOTS = 4
PLANES = 16
PAIR = 2
RANKS = 2


def near(array):
    return pltpu.with_memory_space_constraint(array, pltpu.VMEM)


def far(array):
    return pltpu.with_memory_space_constraint(array, pltpu.HBM)


def iota(shape, dim):
    return lax.broadcasted_iota(jnp.int32, shape, dim)


def one_hot(mask):
    return jnp.where(mask, 1.0, 0.0).astype(jnp.bfloat16)


def dot(left, right):
    return jnp.dot(left, right, preferred_element_type=jnp.float32)


def room(mib):
    return pltpu.CompilerParams(vmem_limit_bytes=mib * 2**20)


def price(flops, nbytes):
    return pl.CostEstimate(flops=flops, bytes_accessed=nbytes, transcendentals=0)


def turned(array, cosine, sine):
    half = HEAD // 2
    front, back = array[:half], array[half:]
    return jnp.concatenate(
        [front * cosine - back * sine, back * cosine + front * sine], 0
    ).astype(jnp.bfloat16)


def over_rows(left, right):
    return lax.dot_general(left, right, (((0,), (0,)), ((), ())), preferred_element_type=jnp.float32)


def attend_kernel(
    core_ref, edge_ref, sink_ref, query_ref, key_ref, value_ref, rim_ref, *refs
):
    count = query_ref.shape[0]
    cosine_ref, sine_ref, weight_hbm, out_ref, weight_ref, fetched = refs
    fetch = pltpu.make_async_copy(weight_hbm, weight_ref, fetched)
    fetch.start()
    cosine, sine = cosine_ref[...], sine_ref[...]
    keys = jnp.concatenate([rim_ref[:HEAD], key_ref[...]], 1).astype(jnp.float32)
    keys = turned(keys, cosine, sine)
    values = jnp.concatenate([rim_ref[HEAD:], value_ref[...]], 1)
    queries = query_ref[...].astype(jnp.float32).T
    cosine, sine = cosine[:, WINDOW:], sine[:, WINDOW:]
    queries = [turned(queries[at : at + HEAD], cosine, sine) for at in (0, HEAD)]
    shape = (2 * WINDOW, 2 * WINDOW)
    key_at = lax.broadcasted_iota(jnp.int32, shape, 0)
    query_at = lax.broadcasted_iota(jnp.int32, shape, 1) & (WINDOW - 1)
    seen = (key_at > query_at) & (key_at <= query_at + WINDOW)
    first_head = lax.broadcasted_iota(jnp.int32, (1, 2 * WINDOW), 1) < WINDOW
    sink = jnp.where(first_head, sink_ref[0], sink_ref[1])
    for at in range(0, count, WINDOW):
        here = jnp.concatenate([q[:, at : at + WINDOW] for q in queries], 1)
        scores = over_rows(keys[:, at : at + 2 * WINDOW], here) * HEAD ** (-0.5)
        allowed = seen
        if at == 0:
            allowed = allowed & (key_at >= edge_ref[0])
        scores = jnp.where(allowed, scores, -jnp.inf)
        highest = jnp.maximum(jnp.max(scores, 0, keepdims=True), sink)
        raised = jnp.exp(scores - highest)
        denominator = jnp.sum(raised, 0, keepdims=True) + jnp.exp(sink - highest)
        weighted = jnp.dot(
            values[:, at : at + 2 * WINDOW],
            raised.astype(jnp.bfloat16),
            preferred_element_type=jnp.float32,
        )
        attended = (weighted / denominator).astype(jnp.bfloat16)
        attended = jnp.concatenate([attended[:, :WINDOW], attended[:, WINDOW:]], 0)
        if at == 0:
            fetch.wait()
        share = over_rows(attended, weight_ref[...]).astype(jnp.bfloat16)
        rows = out_ref.shape[1]
        for k in range(WINDOW // rows):
            owner = at // rows + k
            to = jnp.where(core_ref[0] == 0, *(order.index(owner) for order in ORDERS))
            out_ref[to] = share[k * rows : (k + 1) * rows]


def attention_share(core, edge, sinks, queries, keys_t, values_t, rim, angles, weight, chips):
    count, width = queries.shape[0], weight.shape[1]
    return pl.pallas_call(
        attend_kernel,
        out_shape=jax.ShapeDtypeStruct((chips, count // chips, width), jnp.bfloat16),
        in_specs=[IN_SMEM] * 3 + [IN_VMEM] * 6 + [IN_HBM],
        out_specs=IN_VMEM,
        scratch_shapes=[pltpu.VMEM(weight.shape, weight.dtype), pltpu.SemaphoreType.DMA],
        cost_estimate=pl.CostEstimate(
            flops=2 * count * 128 * (width + 1024),
            bytes_accessed=2 * (count + 128) * width,
            transcendentals=2 * count * 256,
        ),
    )(core, edge, sinks, queries, keys_t, values_t, *map(near, (rim, *angles)), far(weight))


def rim_kernel(key_ref, value_ref, out_ref, sems):
    copies = [
        pltpu.make_async_copy(
            ref.at[:, pl.ds(ref.shape[1] - WINDOW, WINDOW)],
            out_ref.at[pl.ds(k * HEAD, HEAD)],
            sems.at[k],
        )
        for k, ref in enumerate((key_ref, value_ref))
    ]
    for copy in copies:
        copy.start()
    for copy in copies:
        copy.wait()


def rim_of(keys_t, values_t):
    return pl.pallas_call(
        rim_kernel,
        out_shape=pltpu.VMEM((2 * HEAD, WINDOW), keys_t.dtype),
        in_specs=[IN_HBM] * 2,
        out_specs=IN_VMEM,
        scratch_shapes=[pltpu.SemaphoreType.DMA((2,))],
        cost_estimate=price(10**5, 2**16),
    )(far(keys_t), far(values_t))


def plan_kernel(ids_ref, ids_row_ref, spread_ref, collect_ref):
    rows, picks = ids_ref.shape
    lines = collect_ref.shape[2]
    below, right = iota((rows, rows), 0), iota((rows, rows), 1)
    spread = [jnp.zeros((lines, rows), jnp.float32)] * 2
    for k in range(picks):
        col, row = ids_ref[:, k : k + 1], ids_row_ref[k : k + 1, :]
        rank_col = jnp.zeros((rows, 1), jnp.int32)
        rank_row = jnp.zeros((1, rows), jnp.int32)
        for j in range(picks):
            other_col, other_row = ids_ref[:, j : j + 1], ids_row_ref[j : j + 1, :]
            before = jnp.where((col == other_row) & (right < below), 1, 0)
            rank_col = rank_col + jnp.sum(before, 1, keepdims=True)
            before = jnp.where((other_col == row) & (below < right), 1, 0)
            rank_row = rank_row + jnp.sum(before, 0, keepdims=True)
        for half in range(2):
            line_col = (col >> 1) * LINES + half * SLOTS + (col & 1) * RANKS + rank_col
            line_row = (row >> 1) * LINES + half * SLOTS + (row & 1) * RANKS + rank_row
            collect_ref[half, k * rows : (k + 1) * rows, :] = one_hot(
                iota((rows, lines), 1) == line_col
            )
            spread[half] = spread[half] + jnp.where(
                iota((lines, rows), 0) == line_row, 1.0, 0.0
            )
    for half in range(2):
        spread_ref[half] = spread[half].astype(jnp.bfloat16)


def plan(ids):
    rows, picks = ids.shape
    lines = PLANES * LINES
    return pl.pallas_call(
        plan_kernel,
        out_shape=(
            jax.ShapeDtypeStruct((2, lines, rows), jnp.bfloat16),
            jax.ShapeDtypeStruct((2, picks * rows, lines), jnp.bfloat16),
        ),
        in_specs=[IN_VMEM] * 2,
        out_specs=[IN_VMEM] * 2,
        compiler_params=room(16),
        cost_estimate=price(10**6, 2**14),
    )(ids, ids.T)


def pack_kernel(gate_ref, up_ref, down_ref, *refs):
    *out_refs, sems = refs
    copies = []
    for half, out_ref in enumerate(out_refs):
        lanes = pl.ds(half * 128, 128)
        pieces = [
            (gate_ref.at[:, :, lanes], out_ref.at[0]),
            (up_ref.at[:, :, lanes], out_ref.at[1]),
        ]
        for j in range(out_ref.shape[1]):
            pieces.append((down_ref.at[lanes, pl.ds(j * 128, 128)], out_ref.at[2, j]))
        for k, (source, target) in enumerate(pieces):
            copies.append(pltpu.make_async_copy(source, target, sems.at[half, k]))
    for copy in copies:
        copy.start()
    for copy in copies:
        copy.wait()


def pack(gate, up, down):
    units, width = down.shape
    blocks = width // 128
    shape = jax.ShapeDtypeStruct((3, blocks, 128, units // 2), jnp.bfloat16)
    return pl.pallas_call(
        pack_kernel,
        out_shape=(shape, shape),
        in_specs=[IN_HBM] * 3,
        out_specs=[IN_VMEM] * 2,
        scratch_shapes=[pltpu.SemaphoreType.DMA((2, 2 + blocks))],
        cost_estimate=price(10**6, 12 * units * width),
    )(*map(far, (gate.reshape(blocks, 128, units), up.reshape(blocks, 128, units), down)))


def hold_kernel(in_ref, out_ref):
    out_ref[...] = in_ref[...]


def hold(array):
    return pl.pallas_call(
        hold_kernel,
        out_shape=jax.ShapeDtypeStruct(array.shape, array.dtype),
        in_specs=[IN_VMEM],
        out_specs=IN_VMEM,
        compiler_params=room(4),
        cost_estimate=price(10**6, 2**13),
    )(array)


def settle_kernel(shares_ref, residual_ref, gain_ref, spread_ref, middle_ref, out_ref):
    projected = jnp.sum(shares_ref[...].astype(jnp.float32), 0)
    middle = (residual_ref[...].astype(jnp.float32) + projected).astype(jnp.bfloat16)
    middle_ref[...] = middle
    middle = middle.astype(jnp.float32)
    square = jnp.mean(middle * middle, -1, keepdims=True)
    normed = (middle * lax.rsqrt(square + norm_epsilon) * gain_ref[...]).astype(jnp.bfloat16)
    half = normed.shape[1] // 2
    lines = dot(spread_ref[0], normed[:, :half]) + dot(spread_ref[1], normed[:, half:])
    out_ref[...] = lines.astype(jnp.bfloat16)


def settle(shares, residual, gain, spread):
    rows, width = residual.shape
    lines = spread.shape[1]
    return pl.pallas_call(
        settle_kernel,
        out_shape=(
            jax.ShapeDtypeStruct((rows, width), jnp.bfloat16),
            jax.ShapeDtypeStruct((lines, width // 2), jnp.bfloat16),
        ),
        in_specs=[IN_VMEM] * 4,
        out_specs=[IN_VMEM] * 2,
        compiler_params=room(16),
        cost_estimate=price(2 * lines * rows * width, 2 * shares.size),
    )(near(shares), residual, gain, near(spread))


def lines_of(half):
    shape = (PAIR * PLANES * RANKS, PLANES * LINES)
    row = iota(shape, 0)
    per_expert = PLANES * RANKS
    plane, slot = (row % per_expert) // RANKS, row // per_expert * RANKS + row % RANKS
    return iota(shape, 1) == plane * LINES + half * SLOTS + slot


def for_each_core(core_ref, body):
    for core in range(2):

        @pl.when(core_ref[0] == core)
        def _():
            body(core)


def fan_kernel(core_ref, lines_ref, out_ref):
    half = lines_ref.shape[1]
    count = out_ref.shape[1]
    for h in range(2):
        rows = dot(one_hot(lines_of(h)), lines_ref[...]).astype(jnp.bfloat16)

        def hand_out(core):
            for to in range(out_ref.shape[0]):
                at = column_parity(to, core) * count
                out_ref[to, :, h * half : (h + 1) * half] = rows[at : at + count]

        for_each_core(core_ref, hand_out)


def fan(core, lines, chips):
    rows, width = PLANES * RANKS, 2 * lines.shape[1]
    return pl.pallas_call(
        fan_kernel,
        out_shape=jax.ShapeDtypeStruct((chips, rows, width), jnp.bfloat16),
        in_specs=[IN_SMEM, IN_VMEM],
        out_specs=IN_VMEM,
        compiler_params=room(16),
        cost_estimate=price(8 * rows * lines.size, 2 * chips * rows * width),
    )(core, near(lines))


def fold_kernel(core_ref, parts_ref, out_ref, rows_ref):
    half = out_ref.shape[1]
    count = parts_ref.shape[1]

    def add_up(core):
        totals = [0.0] * PAIR
        for chip in range(parts_ref.shape[0]):
            expert = column_parity(chip, core)
            totals[expert] = totals[expert] + parts_ref[chip].astype(jnp.float32)
        for expert, total in enumerate(totals):
            rows_ref[expert * count : (expert + 1) * count] = total.astype(jnp.bfloat16)

    for_each_core(core_ref, add_up)
    lines = 0.0
    for h in range(2):
        lines = lines + over_rows(one_hot(lines_of(h)), rows_ref[:, h * half : (h + 1) * half])
    out_ref[...] = lines.astype(jnp.bfloat16)


def fold(core, parts):
    _, rows, width = parts.shape
    lines = PLANES * LINES
    return pl.pallas_call(
        fold_kernel,
        out_shape=jax.ShapeDtypeStruct((lines, width // 2), jnp.bfloat16),
        in_specs=[IN_SMEM, IN_VMEM],
        out_specs=IN_VMEM,
        scratch_shapes=[pltpu.VMEM((PAIR * rows, width), jnp.bfloat16)],
        compiler_params=room(24),
        cost_estimate=price(2 * lines * PAIR * rows * width, 2 * parts.size),
    )(core, near(parts))


def finish_kernel(lines_ref, collect_ref, share_ref, middle_ref, out_ref):
    rows = middle_ref.shape[0]
    half = lines_ref.shape[1]
    for h in range(2):
        at = slice(h * half, (h + 1) * half)
        picked = dot(collect_ref[h], lines_ref[...])
        routed = picked[:rows] * share_ref[:, :1] + picked[rows:] * share_ref[:, 1:]
        out_ref[:, at] = (middle_ref[:, at].astype(jnp.float32) + routed).astype(jnp.bfloat16)


def finish(lines, collect, shares, middle):
    return pl.pallas_call(
        finish_kernel,
        out_shape=jax.ShapeDtypeStruct(middle.shape, middle.dtype),
        in_specs=[IN_VMEM] * 4,
        out_specs=IN_VMEM,
        compiler_params=room(16),
        cost_estimate=price(4 * collect.size * lines.shape[1], 4 * lines.size),
    )(*map(near, (lines, collect)), shares, near(middle))


def expert_kernel(kept_ref, rows_ref, *refs):
    own, turned, passed = refs[0:2], refs[2:4], refs[4:6]
    out_ref, *slots, sems = refs[6:]
    gates, ups, downs = slots
    kept = kept_ref[0] == 1
    halves = range(len(own))

    def copy(source, slot, kind, half):
        units = pl.ds(half * 128, 128)
        place = (slot, slice(None), units) if kind == 2 else (slot, slice(None), slice(None), units)
        target = slots[kind].at[place]
        return pltpu.make_async_copy(source[half].at[kind], target, sems.at[slot, kind, half])

    def fetch(slot, kind):
        if slot == 0:
            for half in halves:
                copy(turned, slot, kind, half).start()
            return

        @pl.when(kept)
        def _():
            for half in halves:
                copy(own, slot, kind, half).start()

        @pl.when(jnp.logical_not(kept))
        def _():
            for half in halves:
                copy(passed, slot, kind, half).start()

    def ready(slot, kinds):
        for kind in kinds:
            for half in halves:
                copy(turned, slot, kind, half).wait()

    for slot, kind in ((0, 0), (0, 1), (1, 0), (1, 1), (0, 2), (1, 2)):
        fetch(slot, kind)
    rows = rows_ref[...]
    hidden = []
    for slot in range(2):
        ready(slot, (0, 1))
        gate_val = dot(rows, gates[slot].reshape(rows.shape[1], -1))
        up_val = dot(rows, ups[slot].reshape(rows.shape[1], -1))
        hidden.append((gate_val / (1.0 + jnp.exp(-gate_val)) * up_val).astype(jnp.bfloat16))
    ready(0, (2,))
    ready(1, (2,))
    chunk = 512
    for at in range(0, out_ref.shape[1], chunk):
        total = 0.0
        for slot in range(2):
            blocks = [downs[slot, j] for j in range(at // 128, (at + chunk) // 128)]
            total = total + dot(hidden[slot], jnp.concatenate(blocks, 1))
        out_ref[:, at : at + chunk] = total.astype(jnp.bfloat16)


def expert_part(kept, rows, own, turned, passed):
    count, width = rows.shape
    _, blocks, lanes, half = own[0].shape
    return pl.pallas_call(
        expert_kernel,
        out_shape=pltpu.VMEM((count, width), jnp.bfloat16),
        in_specs=[IN_SMEM, IN_VMEM] + [IN_HBM] * 6,
        out_specs=IN_VMEM,
        scratch_shapes=[
            pltpu.VMEM((2, blocks, lanes, 2 * half), jnp.bfloat16),
            pltpu.VMEM((2, blocks, lanes, 2 * half), jnp.bfloat16),
            pltpu.VMEM((2, blocks, 2 * half, lanes), jnp.bfloat16),
            pltpu.SemaphoreType.DMA((2, 3, 2)),
        ],
        compiler_params=room(32),
        cost_estimate=pl.CostEstimate(
            flops=24 * count * half * width,
            bytes_accessed=4 * count * width + 24 * half * width,
            transcendentals=4 * count * half,
        ),
    )(kept, near(rows), *map(far, (*own, *turned, *passed)))


def per_device(
    queries,
    key_rows,
    values,
    sink_logits,
    residual,
    out_weight,
    norm_gain,
    expert_ids,
    route_weight,
    gate_proj,
    up_proj,
    down_proj,
):
    local_len = queries.shape[0]
    span = lax.axis_index(SP)
    core = lax.axis_index("core")
    core_at = core.astype(jnp.int32).reshape(1)
    chips = lax.axis_size(TP)
    keys_t, values_t = key_rows.T, values.T
    rim = from_behind(rim_of(keys_t, values_t), SP, 1)
    half = HEAD // 2
    frequency = 10000.0 ** (-jnp.arange(half, dtype=jnp.float32) * 2.0 / HEAD)
    positions = span * local_len - WINDOW + jnp.arange(local_len + WINDOW, dtype=jnp.int32)
    angles = positions.astype(jnp.float32)[None, :] * frequency[:, None]
    angles = (jnp.cos(angles), jnp.sin(angles))
    edge = jnp.where(span == 0, WINDOW, 0).astype(jnp.int32).reshape(1)
    shares = attention_share(
        core_at, edge, sink_logits, queries, keys_t, values_t, rim, angles, out_weight, chips
    )
    tok_rows, width = residual.shape
    first = lax.axis_index(TP) * tok_rows
    own_ids = lax.dynamic_slice_in_dim(expert_ids, first, tok_rows, 0)
    own_weights = lax.dynamic_slice_in_dim(route_weight, first, tok_rows, 0)
    shares = in_plane(shares)
    own = pack(gate_proj[0], up_proj[0], down_proj[0])
    right = turn(own[0], 1)
    left = turn(own[1], -1)
    spread, collect = plan(own_ids)
    middle, lines = settle(shares, residual, norm_gain.reshape(1, -1), spread)
    lines = along_z(lines.reshape(PLANES, LINES, width // 2))
    fanned = fan(core_at, lines.reshape(PLANES * LINES, width // 2), chips)
    gathered = in_plane(fanned)
    right_too = pass_on(right)
    left_too = pass_on(left)
    kept = (core == lax.axis_index("x") % 2).astype(jnp.int32).reshape(1)
    own_weights = hold(own_weights)
    parts = expert_part(
        kept, gathered.reshape(-1, width), own, (right, left), (right_too, left_too)
    )
    parts = in_plane(parts.reshape(chips, -1, width))
    lines = fold(core_at, parts)
    lines = along_z(lines.reshape(PLANES, LINES, width // 2))
    return finish(lines.reshape(PLANES * LINES, width // 2), collect, own_weights, middle)


def solution(mesh):
    fine = jax.sharding.Mesh(mesh.devices.reshape(SIZES), SP + TP)
    return jax.shard_map(
        per_device,
        mesh=fine,
        in_specs=(
            P(SP, TP),
            P(SP, TP),
            P(SP, TP),
            P(TP),
            P(SP + TP, None),
            P(TP, None),
            P(),
            P(SP, None),
            P(SP, None),
            P(SP, None, TP),
            P(SP, None, TP),
            P(SP, TP, None),
        ),
        out_specs=P(SP + TP, None),
        check_vma=False,
    )
```
